512 devices in a mesh: sp: 128 (over z, y, core), tp: 4 (over x).
Axes of the slice: x: 4, y: 8, z: 8, core: 2. Of those that a mesh axis runs over, the one named last changes fastest.
Arguments:
- inputs: bfloat16 [2, 16384, 2048], P(None, 'sp'), may hold values from -6 to 6
- norm_gain: float32 [2048], replicated, may hold values from 0.1 to 1.9
- query_weight: bfloat16 [2048, 1024], P('sp', 'tp'), may hold values from -0.125 to 0.125
- key_weight: bfloat16 [2048, 256], P('sp', 'tp'), may hold values from -0.125 to 0.125
- value_weight: bfloat16 [2048, 256], P('sp', 'tp'), may hold values from -0.125 to 0.125
- query_gain: float32 [64], replicated, may hold values from 0.1 to 24
- key_gain: float32 [64], replicated, may hold values from 0.1 to 1.9
- forget_cache: float32 [2, 16, 16384], P(None, 'tp'), may hold values from -1640 to 0, as said below
- rec_in_weight: bfloat16 [2048, 1024], P('sp', 'tp'), may hold values from -0.125 to 0.125
- rec_gate_weight: bfloat16 [2048, 1024], P('sp', 'tp'), may hold values from -0.125 to 0.125
- conv_weight: bfloat16 [4, 1024], P(None, 'tp'), may hold values from -3 to 3
- decay_gate_weight: bfloat16 [16, 64, 64], P('tp'), may hold values from -0.75 to 0.75
- input_gate_weight: bfloat16 [16, 64, 64], P('tp'), may hold values from -0.75 to 0.75
- decay_param: float32 [1024], P('tp'), may hold values from 4 to 16
- decay_extra: float32 [2, 16384, 1024], P(None, 'sp', 'tp'), may hold values from -2 to 0
- attn_out_gain: float32 [1024], P('tp'), may hold values from 0.1 to 1.9
- rec_out_gain: float32 [1024], P('tp'), may hold values from 0.1 to 1.9
- out_att_weight: bfloat16 [1024, 2048], P('tp'), may hold values from -0.125 to 0.125
- out_rec_weight: bfloat16 [1024, 2048], P('tp'), may hold values from -0.125 to 0.125
Outputs:
- mixed: bfloat16 [2, 16384, 2048], P(None, 'sp', 'tp')
The draws below stay inside these ranges and needn't reach their ends.
Inputs may be any that keep to these rules, and one draw needn't show every extreme that they name: `forget_cache`: Non-increasing along the positions of each sequence and head.
All inputs are finite; a program needn't handle non-finite values.
Results may differ from the reference program's by a relative error of at most 0.012.
The reference program's roundings to bfloat16 on the way count: a program that leaves them out, or rounds other values in their place, can miss the bound.
Values may be sent and summed in bfloat16 or wider, within the bound.
A program may use at most 128 MiB of HBM per device.

```python
import math
import jax
import jax.numpy as jnp
from jax import lax

D = 2048
HEAD_DIM = 64
ATT_HEADS = 16
KV_HEADS = 4
LRU_BLOCK = 64
CONV_TAPS = 4
SEQS = 2
SEQ_TOK = 128
SEQUENCE_LENGTH = 16384
ATT_WIDTH = 1024
KV_WIDTH = 256
LRU_WIDTH = 1024
LRU_BLOCKS = 16


lru_const = 8.0


def spike_log_values(key, total_count):
    key_rows = jax.random.split(key, 2)
    spots = jax.random.randint(key_rows[0], (SEQS, total_count), 0, SEQUENCE_LENGTH)
    kept = jax.random.uniform(key_rows[1], (SEQS, total_count), jnp.float32, 0.5, 0.8)
    hits = (jnp.arange(SEQUENCE_LENGTH)[None, None, :] == spots[:, :, None]).astype(jnp.float32)
    return jnp.sum(hits * jnp.log(kept)[:, :, None], axis=1)


def block_factor(key):
    blocks = SEQUENCE_LENGTH // SEQ_TOK
    multiplier = jnp.exp(jax.random.uniform(key, (SEQS, blocks), jnp.float32, math.log(0.5), math.log(2.0)))
    return jnp.repeat(multiplier, SEQ_TOK, axis=1)


def draw_query_gain(key, part):
    key = jax.random.fold_in(key, 3)
    return 1.0 + 0.18 * jnp.clip(jax.random.normal(key, (HEAD_DIM,), jnp.float32), -4.5, 4.5)


def draw_forget_cache(key, part):
    key_rows = jax.random.split(jax.random.fold_in(key, 7), 6)
    order = jax.random.permutation(key_rows[0], ATT_HEADS)
    slow_rate = 0.6 / SEQUENCE_LENGTH * jax.random.uniform(key_rows[1], (ATT_HEADS,), jnp.float32, 0.5, 1.5)
    fast_len = jnp.exp(jax.random.uniform(key_rows[2], (ATT_HEADS,), jnp.float32, math.log(30.0), math.log(100.0)))
    decay_speed = jnp.where(order < ATT_HEADS // 2, 1.0 / fast_len, slow_rate)
    random_jitter = jax.random.uniform(key_rows[4], (SEQS, ATT_HEADS, SEQUENCE_LENGTH), jnp.float32, 0.5, 1.5)
    multiplier = block_factor(key_rows[3])
    gate_logarithm = -decay_speed[None, :, None] * multiplier[:, None, :] * random_jitter + spike_log_values(key_rows[5], 2)[:, None, :]
    return jnp.cumsum(gate_logarithm, axis=2)


def draw_decay_param(key, part):
    key_rows = jax.random.split(jax.random.fold_in(key, 5), 3)
    order = jax.random.permutation(key_rows[0], LRU_WIDTH)
    slow_rate = 0.3 / (lru_const * SEQUENCE_LENGTH) * jax.random.uniform(key_rows[1], (LRU_WIDTH,), jnp.float32, 0.5, 1.5)
    fast_len = jnp.exp(jax.random.uniform(key_rows[2], (LRU_WIDTH,), jnp.float32, math.log(30.0), math.log(100.0)))
    fast_rate = 1.0 / (0.5 * lru_const * fast_len)
    decay_speed = jnp.where(order < LRU_WIDTH // 2, fast_rate, slow_rate)
    return -jnp.log(jnp.expm1(decay_speed))


def draw_decay_extra(key, part):
    key_rows = jax.random.split(jax.random.fold_in(key, 9), 3)
    multiplier = block_factor(key_rows[0])
    random_jitter = jax.random.uniform(key_rows[1], (SEQS, SEQUENCE_LENGTH, LRU_WIDTH), jnp.float32, 0.5, 1.5)
    return -0.5 / SEQUENCE_LENGTH * multiplier[:, :, None] * random_jitter + spike_log_values(key_rows[2], 2)[:, :, None]


def block_scale(stream_key, dims, pieces, low, largest):
    loudness, own = 1.0, jax.random.fold_in(stream_key, 6)
    for dim, shards_of in pieces:
        draws = jnp.exp(jax.random.uniform(jax.random.fold_in(own, dim), (shards_of,), jnp.float32, low / len(pieces), largest / len(pieces)))
        loudness = loudness * jnp.repeat(draws, dims[dim] // shards_of).reshape([-1 if axis == dim else 1 for axis in range(len(dims))])
    return loudness


def normal_values(stream_key, extent, width, limit, shards=(), kind=jnp.bfloat16):
    result = width * jax.random.normal(stream_key, extent, jnp.float32)
    if shards:
        result = result * block_scale(stream_key, extent, shards, -0.22, 0.18)
    return jnp.clip(result, -limit, limit).astype(kind)


def setup_inputs(seed: int = 0) -> dict:
    key_of = jax.random.split(jax.random.key(seed), 20)
    inputs = normal_values(key_of[0], (SEQS, SEQUENCE_LENGTH, D), 1.0, 6.0, ((1, 128),))
    norm_gain = jnp.clip(1.0 + 0.18 * jax.random.normal(key_of[1], (D,), jnp.float32), 0.1, 1.9)
    query_weight = normal_values(key_of[2], (D, ATT_WIDTH), D ** -0.5, 0.125, ((0, 128), (1, 4)))
    key_weight = normal_values(key_of[3], (D, KV_WIDTH), D ** -0.5, 0.125, ((0, 128), (1, 4)))
    value_weight = normal_values(key_of[4], (D, KV_WIDTH), D ** -0.5, 0.125, ((0, 128), (1, 4)))
    query_gain = draw_query_gain(jax.random.fold_in(key_of[19], 71), 0)
    key_gain = jnp.clip(1.0 + 0.18 * jax.random.normal(key_of[6], (HEAD_DIM,), jnp.float32), 0.1, 1.9)
    forget_cache = draw_forget_cache(jax.random.fold_in(key_of[19], 71), 0)
    rec_in_weight = normal_values(key_of[8], (D, LRU_WIDTH), D ** -0.5, 0.125, ((0, 128), (1, 4)))
    rec_gate_weight = normal_values(key_of[9], (D, LRU_WIDTH), D ** -0.5, 0.125, ((0, 128), (1, 4)))
    conv_weight = normal_values(key_of[10], (CONV_TAPS, LRU_WIDTH), CONV_TAPS ** -0.5, 3.0, ((1, 4),))
    decay_gate_weight = normal_values(key_of[11], (LRU_BLOCKS, LRU_BLOCK, LRU_BLOCK), LRU_BLOCK ** -0.5, 0.75, ((0, 4),))
    input_gate_weight = normal_values(key_of[12], (LRU_BLOCKS, LRU_BLOCK, LRU_BLOCK), LRU_BLOCK ** -0.5, 0.75, ((0, 4),))
    decay_param = draw_decay_param(jax.random.fold_in(key_of[19], 71), 0)
    decay_extra = draw_decay_extra(jax.random.fold_in(key_of[19], 71), 0)
    attn_out_gain = jnp.clip(1.0 + 0.18 * jax.random.normal(key_of[15], (ATT_WIDTH,), jnp.float32), 0.1, 1.9)
    rec_out_gain = jnp.clip(1.0 + 0.18 * jax.random.normal(key_of[16], (LRU_WIDTH,), jnp.float32), 0.1, 1.9)
    out_att_weight = normal_values(key_of[17], (ATT_WIDTH, D), D ** -0.5, 0.125, ((0, 4),))
    out_rec_weight = normal_values(key_of[18], (LRU_WIDTH, D), D ** -0.5, 0.125, ((0, 4),))
    return {"inputs": inputs, "norm_gain": norm_gain, "query_weight": query_weight, "key_weight": key_weight, "value_weight": value_weight, "query_gain": query_gain, "key_gain": key_gain, "forget_cache": forget_cache, "rec_in_weight": rec_in_weight, "rec_gate_weight": rec_gate_weight, "conv_weight": conv_weight, "decay_gate_weight": decay_gate_weight, "input_gate_weight": input_gate_weight, "decay_param": decay_param, "decay_extra": decay_extra, "attn_out_gain": attn_out_gain, "rec_out_gain": rec_out_gain, "out_att_weight": out_att_weight, "out_rec_weight": out_rec_weight}


lru_const = 8.0
norm_eps = 1e-06

def rms_scale(values, gain):
    multiplier = lax.rsqrt(lax.optimization_barrier(jnp.mean(values * values, axis=-1, keepdims=True)) + norm_eps)
    return values * multiplier * gain

def merge_state(earlier, later):
    return (earlier[0] * later[0], later[0] * earlier[1] + later[1])

def attention(queries, key_heads, value_heads, forget_cache):
    seq_count, kv_count, head_group, length, head_dim = queries.shape
    block_size = 512
    while length % block_size:
        block_size //= 2
    scaling = head_dim ** (-0.5)
    gates = forget_cache.reshape(seq_count, kv_count, head_group, length)
    offsets = jnp.arange(block_size, dtype=jnp.int32)

    def one_block(index):
        first = index * block_size
        query_block = lax.dynamic_slice_in_dim(queries, first, block_size, 3).astype(jnp.float32)
        query_gates = lax.dynamic_slice_in_dim(gates, first, block_size, 3)
        query_pos = first + offsets

        def one_step(block_index, carried):
            top_score, totals, accum = carried
            key_first = block_index * block_size
            key_block = lax.dynamic_slice_in_dim(key_heads, key_first, block_size, 2).astype(jnp.float32)
            value_block = lax.dynamic_slice_in_dim(value_heads, key_first, block_size, 2).astype(jnp.float32)
            key_gates = lax.dynamic_slice_in_dim(gates, key_first, block_size, 3)
            scores = jnp.einsum('bhgqd,bhkd->bhgqk', query_block, key_block) * scaling
            scores = scores + query_gates[..., :, None] - key_gates[..., None, :]
            visible = query_pos[:, None] >= (key_first + offsets)[None, :]
            scores = jnp.where(visible, scores, -jnp.inf)
            new_top = jnp.maximum(top_score, lax.optimization_barrier(jnp.max(scores, axis=-1)))
            weights = jnp.exp(scores - new_top[..., None])
            fading = jnp.exp(top_score - new_top)
            rounded = lax.optimization_barrier(weights.astype(jnp.bfloat16)).astype(jnp.float32)
            totals = totals * fading + lax.optimization_barrier(jnp.sum(weights, axis=-1))
            accum = accum * fading[..., None] + jnp.einsum('bhgqk,bhkd->bhgqd', rounded, value_block)
            return (new_top, totals, accum)
        start_state = (jnp.full((seq_count, kv_count, head_group, block_size), -jnp.inf, jnp.float32), jnp.zeros((seq_count, kv_count, head_group, block_size), jnp.float32), jnp.zeros((seq_count, kv_count, head_group, block_size, head_dim), jnp.float32))
        top_score, totals, accum = lax.fori_loop(0, index + 1, one_step, start_state)
        return accum / totals[..., None]
    return lax.map(one_block, jnp.arange(length // block_size, dtype=jnp.int32))

def reference(inputs, norm_gain, query_weight, key_weight, value_weight, query_gain, key_gain, forget_cache, rec_in_weight, rec_gate_weight, conv_weight, decay_gate_weight, input_gate_weight, decay_param, decay_extra, attn_out_gain, rec_out_gain, out_att_weight, out_rec_weight):
    seq_count, length, model_width = inputs.shape
    row_count = seq_count * length
    head_group = ATT_HEADS // KV_HEADS
    flat_rows = inputs.reshape(row_count, model_width).astype(jnp.float32)
    normed = rms_scale(flat_rows, norm_gain).astype(jnp.bfloat16)

    def project(weight):
        return jnp.dot(normed, weight, preferred_element_type=jnp.float32)
    query_proj = project(query_weight)
    key_proj = project(key_weight)
    gate_proj = project(rec_gate_weight)
    value_proj = project(value_weight).astype(jnp.bfloat16)
    rec_in = project(rec_in_weight).astype(jnp.bfloat16)
    queries = rms_scale(query_proj.reshape(seq_count, length, ATT_HEADS, HEAD_DIM), query_gain).astype(jnp.bfloat16)
    queries = queries.transpose(0, 2, 1, 3).reshape(seq_count, KV_HEADS, head_group, length, HEAD_DIM)
    key_heads = rms_scale(key_proj.reshape(seq_count, length, KV_HEADS, HEAD_DIM), key_gain).astype(jnp.bfloat16)
    key_heads = key_heads.transpose(0, 2, 1, 3)
    value_heads = value_proj.reshape(seq_count, length, KV_HEADS, HEAD_DIM).transpose(0, 2, 1, 3)
    blocks = attention(queries, key_heads, value_heads, forget_cache)
    attended = blocks.transpose(1, 0, 4, 2, 3, 5).reshape(row_count, ATT_HEADS, HEAD_DIM)
    att_normed = rms_scale(attended, attn_out_gain.reshape(ATT_HEADS, HEAD_DIM)).astype(jnp.bfloat16)
    att_normed = att_normed.reshape(row_count, ATT_WIDTH)
    rec_seq = rec_in.reshape(seq_count, length, LRU_WIDTH)
    padded = jnp.pad(rec_seq, ((0, 0), (CONV_TAPS - 1, 0), (0, 0)))
    conv = jnp.zeros((seq_count, length, LRU_WIDTH), jnp.float32)
    for tap in range(CONV_TAPS):
        conv = conv + padded[:, tap:tap + length].astype(jnp.float32) * conv_weight[tap].astype(jnp.float32)
    conv = conv.astype(jnp.bfloat16)
    conv_wide = conv.astype(jnp.float32)
    grouped = conv_wide.reshape(seq_count, length, LRU_BLOCKS, LRU_BLOCK)
    gate_decay = jnp.einsum('bsnd,nde->bsne', grouped, decay_gate_weight.astype(jnp.float32))
    gate_decay = gate_decay.reshape(seq_count, length, LRU_WIDTH)
    gate_input = jnp.einsum('bsnd,nde->bsne', grouped, input_gate_weight.astype(jnp.float32))
    gate_input = gate_input.reshape(seq_count, length, LRU_WIDTH)
    log_decay = -lru_const * jax.nn.sigmoid(gate_decay) * jax.nn.softplus(-decay_param) + decay_extra
    drive = jnp.sqrt(-jnp.expm1(2.0 * log_decay)) * jax.nn.sigmoid(gate_input) * conv_wide
    unused_decay, state = lax.associative_scan(merge_state, (jnp.exp(log_decay), drive), axis=1)
    gated = state * jax.nn.gelu(gate_proj.reshape(seq_count, length, LRU_WIDTH))
    rec_normed = rms_scale(gated.reshape(row_count, LRU_BLOCKS, LRU_BLOCK), rec_out_gain.reshape(LRU_BLOCKS, LRU_BLOCK)).astype(jnp.bfloat16)
    rec_normed = rec_normed.reshape(row_count, LRU_WIDTH)
    mixed = jnp.dot(att_normed, out_att_weight, preferred_element_type=jnp.float32)
    mixed = mixed + jnp.dot(rec_normed, out_rec_weight, preferred_element_type=jnp.float32)
    return mixed.astype(jnp.bfloat16).reshape(seq_count, length, model_width)
```

```python
import functools

import jax
import jax.numpy as jnp
from jax import lax
from jax.experimental import pallas as pl
from jax.experimental.pallas import tpu as pltpu
from jax.sharding import Mesh
from jax.sharding import PartitionSpec as P

D = 2048
LRU_BLOCK = 64
CONV_TAPS = 4
SP = ("sp_0", "sp_1", "sp_2")


lru_const = 8.0
norm_eps = 1e-06


def side_by_side(arrays, axis, dim, along):
    both = jnp.concatenate(arrays, axis=along)
    filled, at, finished = (lax.all_gather(both, axis, axis=dim, tiled=True), 0, [])
    for a in arrays:
        finished.append(lax.slice_in_dim(filled, at, at + a.shape[along], axis=along))
        at += a.shape[along]
    return tuple(finished)


def from_behind(value, axis, steps):
    count = lax.axis_size(axis)
    leading, last = (max(0, -steps), min(count, count - steps))
    return lax.ppermute(value, axis, [(source, source + steps) for source in range(leading, last)])


def filled_with(shard, identity):
    return jax.tree.map(
        lambda a, e: jnp.broadcast_to(jnp.asarray(e, a.dtype), a.shape), shard, identity
    )


def collected_together(shard, axis):
    leaves = jax.tree.leaves(shard)
    order = sorted(range(len(leaves)), key=lambda k: -leaves[k].size)
    width = (1, *leaves[order[0]].shape)[-1]
    lines = [
        jnp.pad(leaves[k].reshape(-1), (0, -leaves[k].size % width)).reshape(-1, width)
        for k in order
    ]
    both, at, found = (lax.all_gather(jnp.concatenate(lines), axis), 0, {})
    for k, line in zip(order, lines):
        share = both[:, at : at + len(line)].reshape(len(both), -1)
        found[k] = share[:, : leaves[k].size].reshape(-1, *leaves[k].shape)
        at += len(line)
    numbers = iter(range(len(leaves)))
    return jax.tree.map(lambda _: found[next(numbers)], shard)


def entering_2(shard, axes, combine, identity):
    before = start = filled_with(shard, identity)
    so_far = shard
    for axis in reversed(axes):
        peers, place = (lax.axis_size(axis), lax.axis_index(axis))
        pieces = collected_together(so_far, axis)
        inside, so_far = (start, start)
        for k in range(peers):
            passed = k < place
            so_far = combine(so_far, jax.tree.map(lambda part: part[k], pieces))
            inside = jax.tree.map(lambda new, old: jnp.where(passed, new, old), so_far, inside)
        before = combine(inside, before)
    return before


def in_blocks(shard, dim, peers):
    dims = shard.shape
    parts = shard.reshape(*dims[:dim], peers, dims[dim] // peers, *dims[dim + 1 :])
    return jnp.moveaxis(parts, dim, 0)


def sent_and_summed(shard, axis, dim):
    peers = lax.axis_size(axis)
    parts = lax.all_to_all(in_blocks(shard, dim, peers), axis, 0, 0, tiled=True)
    return jnp.sum(parts.astype(jnp.float32), axis=0)


def rms_scale(values, gain):
    multiplier = lax.rsqrt(jnp.mean(values * values, axis=-1, keepdims=True) + norm_eps)
    return values * multiplier * gain


def merge_state(earlier, later):
    return (earlier[0] * later[0], later[0] * earlier[1] + later[1])


NT = (((1,), (1,)), ((), ()))

def gate_pieces(rel):
    hi = rel.astype(jnp.bfloat16)
    rest = rel - hi.astype(jnp.float32)
    mid = rest.astype(jnp.bfloat16)
    low = (rest - mid.astype(jnp.float32)).astype(jnp.bfloat16)
    f = jnp.float32
    return jnp.concatenate([hi.astype(f), mid.astype(f), low.astype(f), jnp.zeros_like(rel)], axis=0).astype(jnp.bfloat16)

def attn_kernel(place, CB, q_ref, own_ref, kv_ref, forget_ref, gain_ref, out_ref, gates, acc, top):
    seqs, rows, depth = q_ref.shape
    span = own_ref.shape[2]
    me = place()
    first = pl.multiple_of(me * span, span)
    length = forget_ref.shape[2]
    chunk = CB * span
    ones_own = jnp.ones((16, span), jnp.bfloat16)
    ones = jnp.ones((16, chunk), jnp.bfloat16)
    step = 2048 if length % 2048 == 0 else length
    row = lax.broadcasted_iota(jnp.int32, (rows, span), 0) % span
    col = lax.broadcasted_iota(jnp.int32, (rows, span), 1)
    count = (me + CB - 1) // CB
    for b in range(seqs):
        base = forget_ref[b, :, pl.ds(first, span)][:, :1]
        rel_own = base - forget_ref[b, :, pl.ds(first, span)]
        def prep(c, _):
            at = pl.multiple_of(c * chunk, chunk)
            rel = base - forget_ref[b, :, pl.ds(at, chunk)]
            pos = at + lax.broadcasted_iota(jnp.int32, rel.shape, 1)
            rel = jnp.where(pos < first, rel, -1e30)
            gates[b, :, pl.ds(at, chunk)] = gate_pieces(rel)
            return 0
        lax.fori_loop(0, count, prep, 0)
        own = own_ref[b]
        rhs = jnp.concatenate([own[:64], gate_pieces(rel_own)], axis=0)
        s = jnp.dot(q_ref[b], rhs, preferred_element_type=jnp.float32)
        s = jnp.where(row >= col, s, -jnp.inf)
        m = jnp.max(s, axis=1, keepdims=True)
        p = jnp.exp(s - m).astype(jnp.bfloat16)
        acc[b] = lax.dot_general(p, jnp.concatenate([own[64:], ones_own], axis=0), NT, preferred_element_type=jnp.float32)
        top[b] = jnp.broadcast_to(m, (rows, 128))

    def work(c, _):
        at = pl.multiple_of(c * chunk, chunk)
        for b in range(seqs):
            blocks = [kv_ref[c * CB + i, b] for i in range(CB)]
            kt = jnp.concatenate([x[:64] for x in blocks], axis=1)
            vt = jnp.concatenate([x[64:] for x in blocks], axis=1)
            rhs = jnp.concatenate([kt, gates[b, :, pl.ds(at, chunk)]], axis=0)
            vx = jnp.concatenate([vt, ones], axis=0)
            s = jnp.dot(q_ref[b], rhs, preferred_element_type=jnp.float32)
            old = top[b][:, :1]
            m = jnp.maximum(old, jnp.max(s, axis=1, keepdims=True))
            p = jnp.exp(s - m).astype(jnp.bfloat16)
            fade = jnp.exp(old - m)
            acc[b] = acc[b] * fade + lax.dot_general(p, vx, NT, preferred_element_type=jnp.float32)
            top[b] = jnp.broadcast_to(m, (rows, 128))
        return 0
    lax.fori_loop(0, count, work, 0)
    heads = rows // span
    for b in range(seqs):
        a = acc[b]
        att = a[:, :64] / a[:, 64:65]
        att = att * lax.rsqrt(jnp.mean(att * att, axis=1, keepdims=True) + 1e-6)
        wide = jnp.concatenate([att[h * span:(h + 1) * span] for h in range(heads)], axis=1)
        out_ref[b] = (wide * gain_ref[...]).astype(jnp.bfloat16)

def attention(place, q, own, kv, forget, gain, CB=8):
    seqs, rows, depth = q.shape
    span = own.shape[2]
    length = forget.shape[2]
    heads = rows // span
    return pl.pallas_call(
        functools.partial(attn_kernel, place, CB),
        out_shape=jax.ShapeDtypeStruct((seqs, span, heads * 64), jnp.bfloat16),
        in_specs=[pl.BlockSpec(memory_space=pltpu.VMEM)] * 5,
        out_specs=pl.BlockSpec(memory_space=pltpu.VMEM),
        scratch_shapes=[pltpu.VMEM((seqs, 16, length), jnp.bfloat16), pltpu.VMEM((seqs, rows, 80), jnp.float32), pltpu.VMEM((seqs, rows, 128), jnp.float32)],
        compiler_params=pltpu.CompilerParams(vmem_limit_bytes=60 * 1024 * 1024),
    )(q, own, kv, forget, gain)


def body(
    inputs,
    norm_gain,
    query_weight,
    key_weight,
    value_weight,
    query_gain,
    key_gain,
    forget_cache,
    rec_in_weight,
    rec_gate_weight,
    conv_weight,
    decay_gate_weight,
    input_gate_weight,
    decay_param,
    decay_extra,
    attn_out_gain,
    rec_out_gain,
    out_att_weight,
    out_rec_weight,
):
    seq_count, seq_span, model_width = inputs.shape
    row_count = seq_count * seq_span
    head_dim = query_gain.shape[0]
    att_local = query_weight.shape[1] // head_dim
    kv_local = key_weight.shape[1] // head_dim
    channels = rec_in_weight.shape[1]
    normed = rms_scale(
        inputs.reshape(row_count, model_width).astype(jnp.float32), norm_gain
    ).astype(jnp.bfloat16)
    normed_cols = normed.T
    row_contract = (((0,), (0,)), ((), ()))
    kv_cols = key_weight.shape[1]
    pieces = side_by_side(
        (query_weight, key_weight, value_weight, rec_in_weight, rec_gate_weight), SP, 0, 1
    )
    query_proj, key_proj, value_sum, rec_in_sum, gate_proj = tuple(
        (
            lax.dot_general(
                normed_cols, weight_part, row_contract, preferred_element_type=jnp.float32
            )
            for weight_part in pieces
        )
    )
    queries = rms_scale(query_proj.reshape(row_count, att_local, head_dim), query_gain).astype(
        jnp.bfloat16
    )
    queries = (queries * jnp.bfloat16(head_dim ** (-0.5))).reshape(seq_count, seq_span, att_local, head_dim)
    queries = queries.transpose(0, 2, 1, 3)
    picks = jnp.tile(jnp.eye(att_local, dtype=jnp.bfloat16), (1, 4)) * (jnp.arange(16) < 12).astype(jnp.bfloat16)
    picks = jnp.broadcast_to(picks[None, :, None, :], (seq_count, att_local, seq_span, 16))
    queries = jnp.concatenate([queries, picks], axis=3).reshape(seq_count, att_local * seq_span, head_dim + 16)
    key_heads = rms_scale(key_proj.reshape(row_count, kv_local, head_dim), key_gain).astype(
        jnp.bfloat16
    )
    key_heads = key_heads.reshape(seq_count, seq_span, kv_cols)
    value_heads = value_sum.astype(jnp.bfloat16).reshape(seq_count, seq_span, kv_cols)
    key_value = jnp.concatenate([key_heads, value_heads], axis=2).transpose(0, 2, 1)
    gathered = lax.all_gather(key_value, SP, axis=0)
    att_normed = attention(
        lambda: lax.axis_index(SP), queries, key_value, gathered, forget_cache, attn_out_gain[None], CB=32
    )
    att_normed = att_normed.reshape(row_count, att_local * head_dim)
    rec_in = rec_in_sum.astype(jnp.bfloat16).reshape(seq_count, seq_span, channels)
    before = from_behind(rec_in[:, seq_span - (CONV_TAPS - 1) :, :], SP, 1)
    extended = jnp.concatenate([before, rec_in], axis=1)
    conv = jnp.zeros((seq_count, seq_span, channels), jnp.float32)
    for tap in range(CONV_TAPS):
        conv = conv + extended[:, tap : tap + seq_span].astype(jnp.float32) * conv_weight[
            tap
        ].astype(jnp.float32)
    conv = conv.astype(jnp.bfloat16)
    blocks_local = decay_gate_weight.shape[0]
    grouped = conv.reshape(seq_count, seq_span, blocks_local, LRU_BLOCK)
    gate_decay = jnp.einsum(
        "bsnd,nde->bsne", grouped, decay_gate_weight, preferred_element_type=jnp.float32
    ).reshape(seq_count, seq_span, channels)
    gate_input = jnp.einsum(
        "bsnd,nde->bsne", grouped, input_gate_weight, preferred_element_type=jnp.float32
    ).reshape(seq_count, seq_span, channels)
    log_decay = (
        -lru_const * jax.nn.sigmoid(gate_decay) * jax.nn.softplus(-decay_param) + decay_extra
    )
    drive = (
        jnp.sqrt(-jnp.expm1(2.0 * log_decay))
        * jax.nn.sigmoid(gate_input)
        * conv.astype(jnp.float32)
    )
    cum_decay, local_state = lax.associative_scan(merge_state, (jnp.exp(log_decay), drive), axis=1)
    entering = entering_2(
        (cum_decay[:, seq_span - 1], local_state[:, seq_span - 1]),
        SP,
        merge_state,
        (
            jnp.ones((seq_count, channels), jnp.float32),
            jnp.zeros((seq_count, channels), jnp.float32),
        ),
    )[1]
    state = local_state + cum_decay * entering[:, None, :]
    gated = state * jax.nn.gelu(gate_proj.reshape(seq_count, seq_span, channels))
    rec_normed = rms_scale(
        gated.reshape(row_count, blocks_local, LRU_BLOCK),
        rec_out_gain.reshape(blocks_local, LRU_BLOCK),
    ).astype(jnp.bfloat16)
    rec_normed = rec_normed.reshape(row_count, channels)
    out_cols = D // lax.axis_size("tp")
    pieces = row_count * lax.axis_size("tp") // row_count
    terms = jnp.dot(att_normed, out_att_weight, preferred_element_type=jnp.float32) + jnp.dot(
        rec_normed, out_rec_weight, preferred_element_type=jnp.float32
    )
    mixed_cols = sent_and_summed(
        terms.reshape(row_count, pieces, out_cols)
        .transpose(1, 0, 2)
        .reshape(pieces * row_count, out_cols)
        .astype(jnp.bfloat16),
        "tp",
        0,
    )
    return mixed_cols.astype(jnp.bfloat16).reshape(seq_count, seq_span, out_cols)


def solution(mesh):
    finer = Mesh(mesh.devices.reshape(8, 8, 2, mesh.shape["tp"]), ("sp_0", "sp_1", "sp_2", "tp"))
    return jax.shard_map(
        body,
        mesh=finer,
        in_specs=(
            P(None, SP, None),
            P(),
            P(SP, "tp"),
            P(SP, "tp"),
            P(SP, "tp"),
            P(),
            P(),
            P(None, "tp", None),
            P(SP, "tp"),
            P(SP, "tp"),
            P(None, "tp"),
            P("tp", None, None),
            P("tp", None, None),
            P("tp"),
            P(None, SP, "tp"),
            P("tp"),
            P("tp"),
            P("tp", None),
            P("tp", None),
        ),
        out_specs=P(None, SP, "tp"),
        check_vma=False,
    )
```

```python
import functools

import jax
import jax.numpy as jnp
from jax import lax
from jax.experimental import pallas as pl
from jax.experimental.pallas import tpu as pltpu
from jax.sharding import Mesh
from jax.sharding import PartitionSpec as P

SP = ("sp_0", "sp_1", "sp_2")
NT = (((1,), (1,)), ((), ()))
EPS = 1e-6
HALO = 16
F32, BF16 = jnp.float32, jnp.bfloat16
VMEM = pl.BlockSpec(memory_space=pltpu.VMEM)

MESH = pl.DeviceIdType.MESH
RING = 8


class Torus:
    def __init__(self, streams, sems, subs):
        self.streams, self.subs = streams, subs
        self.s1, self.r1, self.s2, self.r2, self.ps, self.pr = sems
        self.z, self.y, self.c = (lax.axis_index(n) for n in ("sp_0", "sp_1", "sp_2"))
        self.sign = 1 - 2 * self.c
        self.other = {"sp_2": 1 - self.c}
        self.pending = []

    def signals(self):
        z, y = self.z, self.y
        return [
            {"sp_0": lax.rem(z + 1, RING)},
            {"sp_0": lax.rem(z + RING - 1, RING)},
            {"sp_1": lax.rem(y + 1, RING)},
            {"sp_1": lax.rem(y + RING - 1, RING)},
            self.other,
        ]

    def places(self, k):
        return (self.y, self.z) if self.streams[k][2] == "y" else (self.z, self.y)

    def one(self, k, i):
        o, first = self.streams[k][1:]
        return o.at[self.z, i, self.c] if first == "y" else o.at[i, self.y, self.c]

    def many(self, k, i0, n, j, core):
        o, first = self.streams[k][1:]
        return o.at[j, pl.ds(i0, n), core] if first == "y" else o.at[pl.ds(i0, n), j, core]

    def back(self, pos, d, s):
        sg = self.sign if d == 0 else -self.sign
        return lax.rem(pos - sg * s + RING, RING)

    def ahead(self, k, phase, d):
        name = self.streams[k][2]
        first, second = ("sp_1", "sp_0") if name == "y" else ("sp_0", "sp_1")
        pos = self.places(k)[phase]
        return {(first, second)[phase]: self.back(pos, d, -1)}

    def go(self, src, dst, send, recv, device):
        copy = pltpu.make_async_remote_copy(
            src_ref=src, dst_ref=dst, send_sem=send, recv_sem=recv, device_id=device, device_id_type=MESH
        )
        copy.start()
        self.pending.append(copy)

    def arrived(self, ref, send, recv):
        pltpu.make_async_remote_copy(
            src_ref=ref, dst_ref=ref, send_sem=send, recv_sem=recv, device_id=self.other, device_id_type=MESH
        ).wait_recv()

    def steps(self, d):
        return 4 if d == 0 else 3

    def send1(self, k, d, s):
        pos = self.places(k)[0]
        dst = self.one(k, self.back(pos, d, s - 1))
        self.go(self.streams[k][0] if s == 1 else dst, dst, self.s1.at[k, d, s - 1], self.r1.at[k, d, s - 1], self.ahead(k, 0, d))

    def span(self, k, u):
        n = RING // self.subs[k]
        return u * n, n

    def send2(self, k, d, s, u):
        j = self.back(self.places(k)[1], d, s - 1)
        ref = self.many(k, *self.span(k, u), j, self.c)
        self.go(ref, ref, self.s2.at[k, d, s - 1, u], self.r2.at[k, d, s - 1, u], self.ahead(k, 1, d))

    def begin(self):
        for k in range(len(self.streams)):
            for d in (0, 1):
                self.send1(k, d, 1)
        for k in range(len(self.streams)):
            self.streams[k][1][self.z, self.y, self.c] = self.streams[k][0][...]

    def finish(self):
        ks = range(len(self.streams))
        for s in range(1, 5):
            for k in ks:
                for d in (0, 1):
                    if s <= self.steps(d):
                        got = self.one(k, self.back(self.places(k)[0], d, s))
                        self.arrived(got, self.s1.at[k, d, s - 1], self.r1.at[k, d, s - 1])
                        if s < self.steps(d):
                            self.send1(k, d, s + 1)
        for k in ks:
            for u in range(self.subs[k]):
                for d in (0, 1):
                    self.send2(k, d, 1, u)
        for k in ks:
            ref = self.many(k, 0, RING, self.places(k)[1], self.c)
            self.go(ref, ref, self.ps.at[k, 0, 0, 0], self.pr.at[k, 0, 0, 0], self.other)
        for s in range(1, 5):
            for u in range(max(self.subs)):
                for k in ks:
                    if u >= self.subs[k]:
                        continue
                    for d in (0, 1):
                        if s <= self.steps(d):
                            j = self.back(self.places(k)[1], d, s)
                            got = self.many(k, *self.span(k, u), j, self.c)
                            self.arrived(got, self.s2.at[k, d, s - 1, u], self.r2.at[k, d, s - 1, u])
                            if s < self.steps(d):
                                self.send2(k, d, s + 1, u)
                            self.go(got, got, self.ps.at[k, d, s, u], self.pr.at[k, d, s, u], self.other)
        for k in ks:
            ref = self.many(k, 0, RING, self.places(k)[1], 1 - self.c)
            self.arrived(ref, self.ps.at[k, 0, 0, 0], self.pr.at[k, 0, 0, 0])
        for s in range(1, 5):
            for k in ks:
                for u in range(self.subs[k]):
                    for d in (0, 1):
                        if s <= self.steps(d):
                            j = self.back(self.places(k)[1], d, -s)
                            got = self.many(k, *self.span(k, u), j, 1 - self.c)
                            self.arrived(got, self.ps.at[k, d, s, u], self.pr.at[k, d, s, u])
        for copy in self.pending:
            copy.wait_send()


def torus_sems(n, sub):
    dma = pltpu.SemaphoreType.DMA
    return [dma((n, 2, 4)), dma((n, 2, 4)), dma((n, 2, 4, sub)), dma((n, 2, 4, sub)), dma((n, 2, 5, sub)), dma((n, 2, 5, sub))]


def meet(devices):
    barrier = pltpu.get_barrier_semaphore()
    for device in devices:
        pl.semaphore_signal(barrier, inc=1, device_id=device, device_id_type=MESH)
    pl.semaphore_wait(barrier, len(devices))


def params(collective_id=None):
    more = {} if collective_id is None else {"collective_id": collective_id, "has_side_effects": True}
    return pltpu.CompilerParams(vmem_limit_bytes=60 * 1024 * 1024, **more)


def index_of(z, y, c):
    return (z * RING + y) * 2 + c


def coords_of(index):
    return {"sp_0": index // 16, "sp_1": lax.rem(index // 2, RING), "sp_2": lax.rem(index, 2)}


def project_kernel(x_ref, gain_ref, wa_ref, wb_ref, oa_ref, ob_ref, ga, gb, halo, normed, hs, hr, *sems):
    torus = Torus([(wa_ref, ga, "y"), (wb_ref, gb, "z")], sems, (1, 1))
    me = index_of(torus.z, torus.y, torus.c)
    later, earlier = coords_of(lax.rem(me + 1, 128)), coords_of(lax.rem(me + 127, 128))
    meet(torus.signals() + [later, earlier])
    span = x_ref.shape[1]
    torus.go(x_ref.at[:, pl.ds(span - HALO, HALO)], halo, hs, hr, later)
    torus.begin()
    rows = span + HALO

    def norm(values):
        wide = values.astype(F32)
        scale = lax.rsqrt(jnp.mean(wide * wide, axis=-1, keepdims=True) + EPS)
        return (wide * scale * gain_ref[...]).astype(BF16)

    for b in range(2):
        for r in range(0, span, 32):
            normed[b * rows + HALO + r:b * rows + HALO + r + 32] = norm(x_ref[b, r:r + 32])
    torus.arrived(halo, hs, hr)
    for b in range(2):
        normed[b * rows:b * rows + HALO] = norm(halo[b])
    torus.finish()
    depth = normed.shape[1]
    for g, o in ((ga, oa_ref), (gb, ob_ref)):
        o[...] = jnp.dot(normed[...], g[...].reshape(depth, g.shape[-1]), preferred_element_type=F32)


def project(x, gain, wa, wb):
    rows = 2 * (x.shape[1] + HALO)
    dma = pltpu.SemaphoreType.DMA
    return pl.pallas_call(
        project_kernel,
        out_shape=[jax.ShapeDtypeStruct((rows, w.shape[1]), F32) for w in (wa, wb)],
        in_specs=[VMEM] * 4,
        out_specs=[VMEM] * 2,
        scratch_shapes=[
            *[pltpu.VMEM((8, 8, 2, *w.shape), BF16) for w in (wa, wb)],
            pltpu.VMEM((2, HALO, x.shape[2]), BF16),
            pltpu.VMEM((rows, x.shape[2]), BF16),
            dma,
            dma,
            *torus_sems(2, 1),
        ],
        compiler_params=params(0),
    )(x, gain, wa, wb)


def head_scale(values, gain):
    return values * lax.rsqrt(jnp.mean(values * values, axis=-1, keepdims=True) + EPS) * gain


def softplus(values):
    grown = jnp.exp(-jnp.abs(values))
    series = jnp.zeros_like(grown)
    for n in range(8, 0, -1):
        series = grown * ((1.0 if n % 2 else -1.0) / n + series)
    return jnp.maximum(values, 0.0) + jnp.where(grown < 0.06, series, jnp.log(1.0 + grown))


def one_less_exp(values):
    series = jnp.zeros_like(values)
    for n in range(8, 0, -1):
        series = values / n * (1.0 + series)
    return jnp.where(values > -0.3, -series, 1.0 - jnp.exp(values))


def local_kernel(
    oa_ref, ob_ref, qg_ref, kg_ref, cw_ref, dw_ref, iw_ref, dp_ref, de_ref, q_ref, k0_ref, k1_ref, cum_ref, loc_ref, sum_ref
):
    span = q_ref.shape[1] // 4
    rows = span + HALO
    me = lax.axis_index(SP)
    lane = lax.broadcasted_iota(jnp.int32, (span, 16), 1)
    power = softplus(-dp_ref[...]) * -8.0
    for b, k_ref in enumerate((k0_ref, k1_ref)):
        own = pl.ds(b * rows + HALO, span)
        proj = oa_ref[own, :256]
        for h in range(4):
            q = head_scale(proj[:, h * 64:(h + 1) * 64], qg_ref[...]).astype(BF16).astype(F32) * 0.125
            picks = jnp.where((lane % 4 == h) & (lane < 12), 1.0, 0.0)
            q_ref[b, h * span:(h + 1) * span] = jnp.concatenate([q, picks], axis=1).astype(BF16)
        kv = ob_ref[own, :128]
        key = head_scale(kv[:, :64], kg_ref[...])
        k_ref[...] = jnp.concatenate([key, kv[:, 64:]], axis=1).T.astype(BF16)
        before = oa_ref[b * rows:b * rows + HALO, 256:] * jnp.where(me > 0, 1.0, 0.0)
        ext = jnp.concatenate([before, oa_ref[own, 256:]], axis=0).astype(BF16).astype(F32)
        conv = jnp.zeros((span, 256), F32)
        for k in range(4):
            conv = conv + ext[HALO - 3 + k:HALO - 3 + k + span] * cw_ref[k:k + 1].astype(F32)
        conv = conv.astype(BF16)
        gd, gi = (
            jnp.concatenate(
                [jnp.dot(conv[:, n * 64:(n + 1) * 64], w[n], preferred_element_type=F32) for n in range(4)], axis=1
            )
            for w in (dw_ref, iw_ref)
        )
        log_decay = power * jax.nn.sigmoid(gd) + de_ref[b]
        add = jnp.sqrt(one_less_exp(2.0 * log_decay)) * jax.nn.sigmoid(gi) * conv.astype(F32)
        mul = jnp.exp(log_decay)
        s = 1
        while s < span:
            mul_b = jnp.concatenate([jnp.ones((s, 256), F32), mul[:-s]], axis=0)
            add_b = jnp.concatenate([jnp.zeros((s, 256), F32), add[:-s]], axis=0)
            add = mul * add_b + add
            mul = mul * mul_b
            s *= 2
        cum_ref[b] = mul
        loc_ref[b] = add
        sum_ref[0, b:b + 1] = mul[span - 1:]
        sum_ref[1, b:b + 1] = add[span - 1:]


def local(oa, ob, *more):
    span = oa.shape[0] // 2 - HALO
    shape = jax.ShapeDtypeStruct
    return pl.pallas_call(
        local_kernel,
        out_shape=[
            shape((2, 4 * span, 80), BF16),
            *[shape((128, span), BF16)] * 2,
            *[shape((2, span, 256), F32)] * 2,
            shape((2, 2, 256), F32),
        ],
        in_specs=[VMEM] * 9,
        out_specs=[VMEM] * 6,
        compiler_params=params(),
    )(oa, ob, *more)


def gather_kernel(firsts, subs, *refs):
    n = len(firsts)
    torus = Torus([(refs[k], refs[n + k], firsts[k]) for k in range(n)], refs[2 * n:], subs)
    meet(torus.signals())
    torus.begin()
    torus.finish()


def torus_gather(arrays, firsts, subs, collective_id):
    return pl.pallas_call(
        functools.partial(gather_kernel, firsts, subs),
        out_shape=[jax.ShapeDtypeStruct((8, 8, 2, *a.shape), a.dtype) for a in arrays],
        in_specs=[VMEM] * len(arrays),
        out_specs=[VMEM] * len(arrays),
        scratch_shapes=torus_sems(len(arrays), max(subs)),
        compiler_params=params(collective_id),
    )(*arrays)


def gate_pieces(rel):
    hi = rel.astype(BF16).astype(F32)
    mid = (rel - hi).astype(BF16).astype(F32)
    return jnp.concatenate([hi, mid, rel - hi - mid, jnp.zeros_like(rel)], axis=0).astype(BF16)


CB = 32


def mix_kernel(
    q_ref, k0_ref, k1_ref, kv0_ref, kv1_ref, forget_ref, ag_ref, cum_ref, loc_ref, st_ref, ob_ref, rg_ref, wa_ref, wr_ref,
    out_ref, gates, acc, top, normed
):
    seqs, rows, depth = q_ref.shape
    span = k0_ref.shape[1]
    heads = rows // span
    owns, kvs = (k0_ref, k1_ref), (kv0_ref, kv1_ref)
    me = lax.axis_index(SP)
    first = pl.multiple_of(me * span, span)
    chunk = CB * span
    ones_own = jnp.ones((16, span), BF16)
    ones = jnp.ones((16, chunk), BF16)
    row = lax.broadcasted_iota(jnp.int32, (rows, span), 0) % span
    col = lax.broadcasted_iota(jnp.int32, (rows, span), 1)
    count = (me + CB - 1) // CB
    for b in range(seqs):
        near = forget_ref[b, :, pl.ds(first, span)]
        base = near[:, :1]

        def prep(c, _):
            at = pl.multiple_of(c * chunk, chunk)
            rel = base - forget_ref[b, :, pl.ds(at, chunk)]
            pos = at + lax.broadcasted_iota(jnp.int32, rel.shape, 1)
            gates[b, :, pl.ds(at, chunk)] = gate_pieces(jnp.where(pos < first, rel, -1e30))
            return 0

        lax.fori_loop(0, count, prep, 0)
        own = owns[b][...]
        rhs = jnp.concatenate([own[:64], gate_pieces(base - near)], axis=0)
        s = jnp.dot(q_ref[b], rhs, preferred_element_type=F32)
        s = jnp.where(row >= col, s, -jnp.inf)
        m = jnp.max(s, axis=1, keepdims=True)
        p = jnp.exp(s - m).astype(BF16)
        acc[b] = lax.dot_general(p, jnp.concatenate([own[64:], ones_own], axis=0), NT, preferred_element_type=F32)
        top[b] = jnp.broadcast_to(m, (rows, 128))

    def work(c, _):
        at = pl.multiple_of(c * chunk, chunk)
        for b in range(seqs):
            blocks = [kvs[b][c * CB + i] for i in range(CB)]
            kt = jnp.concatenate([x[:64] for x in blocks], axis=1)
            vt = jnp.concatenate([x[64:] for x in blocks], axis=1)
            rhs = jnp.concatenate([kt, gates[b, :, pl.ds(at, chunk)]], axis=0)
            s = jnp.dot(q_ref[b], rhs, preferred_element_type=F32)
            old = top[b][:, :1]
            m = jnp.maximum(old, jnp.max(s, axis=1, keepdims=True))
            p = jnp.exp(s - m).astype(BF16)
            vx = jnp.concatenate([vt, ones], axis=0)
            acc[b] = acc[b] * jnp.exp(old - m) + lax.dot_general(p, vx, NT, preferred_element_type=F32)
            top[b] = jnp.broadcast_to(m, (rows, 128))
        return 0

    lax.fori_loop(0, count, work, 0)

    def merge(j, state):
        return st_ref[j, 0] * state + st_ref[j, 1]

    entering = lax.fori_loop(0, me, merge, jnp.zeros((2, 256), F32))
    wide_rows = span + HALO
    for b in range(seqs):
        a = acc[b]
        att = head_scale(a[:, :64] / a[:, 64:65], 1.0)
        att = jnp.concatenate([att[h * span:(h + 1) * span] for h in range(heads)], axis=1)
        normed[0, b * span:(b + 1) * span] = (att * ag_ref[...]).astype(BF16)
        state = loc_ref[b] + cum_ref[b] * entering[b:b + 1]
        gated = state * jax.nn.gelu(ob_ref[pl.ds(b * wide_rows + HALO, span), 128:])
        rec = jnp.concatenate([head_scale(gated[:, n * 64:(n + 1) * 64], 1.0) for n in range(4)], axis=1)
        normed[1, b * span:(b + 1) * span] = (rec * rg_ref[...]).astype(BF16)
    width = out_ref.shape[2]
    for p in range(4):
        part = pl.ds(p * width, width)
        terms = jnp.dot(normed[0], wa_ref[:, part], preferred_element_type=F32)
        out_ref[p] = (terms + jnp.dot(normed[1], wr_ref[:, part], preferred_element_type=F32)).astype(BF16)


def mix(q, k0, k1, kv0, kv1, forget, *more):
    span, length = k0.shape[1], forget.shape[2]
    rows = q.shape[1]
    return pl.pallas_call(
        mix_kernel,
        out_shape=jax.ShapeDtypeStruct((4, 2 * span, more[-1].shape[1] // 4), BF16),
        in_specs=[VMEM] * (6 + len(more)),
        out_specs=VMEM,
        scratch_shapes=[
            pltpu.VMEM((2, 16, length), BF16),
            pltpu.VMEM((2, rows, 80), F32),
            pltpu.VMEM((2, rows, 128), F32),
            pltpu.VMEM((2, 2 * span, 256), BF16),
        ],
        compiler_params=params(),
    )(q, k0, k1, kv0, kv1, forget, *more)


def sum_kernel(terms_ref, out_ref, held, send, recv):
    me = lax.axis_index("tp")
    peers = [lax.rem(me + j, 4) for j in range(4)]
    meet([{"tp": p} for p in peers[1:]])
    copies = []
    for j in (2, 1, 3):
        copy = pltpu.make_async_remote_copy(
            src_ref=terms_ref.at[peers[j]], dst_ref=held.at[j - 1], send_sem=send.at[j - 1], recv_sem=recv.at[j - 1],
            device_id={"tp": peers[j]}, device_id_type=MESH,
        )
        copy.start()
        copies.append(copy)
    for copy in copies:
        copy.wait()
    total = terms_ref[me].astype(F32)
    for j in range(3):
        total = total + held[j].astype(F32)
    out_ref[...] = total.astype(BF16)


def summed(terms):
    dma = pltpu.SemaphoreType.DMA
    return pl.pallas_call(
        sum_kernel,
        out_shape=jax.ShapeDtypeStruct(terms.shape[1:], BF16),
        in_specs=[VMEM],
        out_specs=VMEM,
        scratch_shapes=[pltpu.VMEM((3, *terms.shape[1:]), BF16), dma((3,)), dma((3,))],
        compiler_params=params(2),
    )(terms)


def body(
    inputs, norm_gain, query_weight, key_weight, value_weight, query_gain, key_gain, forget_cache, rec_in_weight,
    rec_gate_weight, conv_weight, decay_gate_weight, input_gate_weight, decay_param, decay_extra, attn_out_gain,
    rec_out_gain, out_att_weight, out_rec_weight,
):
    span = inputs.shape[1]
    wa = jnp.concatenate([query_weight, rec_in_weight], axis=1)
    wb = jnp.concatenate([key_weight, value_weight, rec_gate_weight], axis=1)
    oa, ob = project(inputs, norm_gain[None], wa, wb)
    q, k0, k1, cum, loc, ends = local(
        oa, ob, query_gain[None], key_gain[None], conv_weight, decay_gate_weight, input_gate_weight, decay_param[None],
        decay_extra,
    )
    kv0, kv1, states = torus_gather([k0, k1, ends], ("y", "z", "y"), (2, 2, 1), 1)
    terms = mix(
        q, k0, k1, kv0.reshape(-1, *k0.shape), kv1.reshape(-1, *k1.shape), forget_cache, attn_out_gain[None], cum, loc,
        states.reshape(-1, *ends.shape), ob, rec_out_gain[None], out_att_weight, out_rec_weight,
    )
    return summed(terms).reshape(2, span, -1)


def solution(mesh):
    finer = Mesh(mesh.devices.reshape(8, 8, 2, mesh.shape["tp"]), (*SP, "tp"))
    return jax.shard_map(
        body,
        mesh=finer,
        in_specs=(
            P(None, SP, None), P(), P(SP, "tp"), P(SP, "tp"), P(SP, "tp"), P(), P(), P(None, "tp", None), P(SP, "tp"),
            P(SP, "tp"), P(None, "tp"), P("tp", None, None), P("tp", None, None), P("tp"), P(None, SP, "tp"), P("tp"),
            P("tp"), P("tp", None), P("tp", None),
        ),
        out_specs=P(None, SP, "tp"),
        check_vma=False,
    )
```

```python
import functools

import jax
import jax.numpy as jnp
from jax import lax
from jax.experimental import pallas as pl
from jax.experimental.pallas import tpu as pltpu
from jax.sharding import Mesh
from jax.sharding import PartitionSpec as P

SP = ("sp_0", "sp_1", "sp_2")
NT = (((1,), (1,)), ((), ()))
EPS = 1e-6
HALO = 16
F32, BF16 = jnp.float32, jnp.bfloat16
VMEM = pl.BlockSpec(memory_space=pltpu.VMEM)

MESH = pl.DeviceIdType.MESH
RING = 8


class Torus:
    def __init__(self, streams, sems):
        self.streams = streams
        self.s1, self.r1, self.s2, self.r2, self.ps, self.pr = sems
        self.z, self.y, self.c = (lax.axis_index(n) for n in SP)
        self.sign = 1 - 2 * self.c
        self.other = {"sp_2": 1 - self.c}
        self.pending = []
        self.ks = range(len(streams))

    def peers(self):
        found = [self.other]
        for name, pos in (("sp_0", self.z), ("sp_1", self.y)):
            found += [{name: lax.rem(pos + i, RING)} for i in range(1, RING)]
        return found

    def places(self, k):
        return (self.y, self.z) if self.streams[k][2] == "y" else (self.z, self.y)

    def axes(self, k):
        return ("sp_1", "sp_0") if self.streams[k][2] == "y" else ("sp_0", "sp_1")

    def one(self, k, i):
        o, first = self.streams[k][1:]
        return o.at[self.z, i, self.c] if first == "y" else o.at[i, self.y, self.c]

    def line(self, k, j, core):
        o, first = self.streams[k][1:]
        return o.at[j, :, core] if first == "y" else o.at[:, j, core]

    def back(self, k, d, s):
        sg = self.sign if d == 0 else -self.sign
        return lax.rem(self.places(k)[1] - sg * s + RING, RING)

    def go(self, src, dst, send, recv, device):
        copy = pltpu.make_async_remote_copy(
            src_ref=src, dst_ref=dst, send_sem=send, recv_sem=recv, device_id=device, device_id_type=MESH
        )
        copy.start()
        self.pending.append(copy)

    def arrived(self, ref, send, recv):
        pltpu.make_async_remote_copy(
            src_ref=ref, dst_ref=ref, send_sem=send, recv_sem=recv, device_id=self.other, device_id_type=MESH
        ).wait_recv()

    def begin(self):
        for i in (4, 5, 3, 6, 2, 7, 1):
            for k in self.ks:
                pos = self.places(k)[0]
                self.go(
                    self.streams[k][0], self.one(k, pos), self.s1.at[k, i - 1], self.r1.at[k, i - 1],
                    {self.axes(k)[0]: lax.rem(pos + i, RING)},
                )
        for k in self.ks:
            self.streams[k][1][self.z, self.y, self.c] = self.streams[k][0][...]

    def pass_on(self, k, d, s):
        j = self.back(k, d, s - 1)
        ref = self.line(k, j, self.c)
        device = {self.axes(k)[1]: self.back(k, d, -1)}
        self.go(ref, ref, self.s2.at[k, d, s - 1], self.r2.at[k, d, s - 1], device)

    def share(self, k, d, s):
        ref = self.line(k, self.back(k, d, s), self.c)
        self.go(ref, ref, self.ps.at[k, d, s], self.pr.at[k, d, s], self.other)

    def shared(self, k, d, s):
        ref = self.line(k, self.back(k, d, -s), 1 - self.c)
        self.arrived(ref, self.ps.at[k, d, s], self.pr.at[k, d, s])

    def finish(self, work=lambda k, j: None):
        for k in self.ks:
            for i in range(1, RING):
                pos = self.places(k)[0]
                got = self.one(k, lax.rem(pos + RING - i, RING))
                self.arrived(got, self.s1.at[k, i - 1], self.r1.at[k, i - 1])
            for d in (0, 1):
                self.pass_on(k, d, 1)
            self.share(k, 0, 0)
        for k in self.ks:
            self.shared(k, 0, 0)
        for k in self.ks:
            work(k, self.places(k)[1])
        for s in range(1, 5):
            for k in self.ks:
                for d in (0, 1):
                    if s + d <= 4:
                        got = self.line(k, self.back(k, d, s), self.c)
                        self.arrived(got, self.s2.at[k, d, s - 1], self.r2.at[k, d, s - 1])
                        if s + d < 4:
                            self.pass_on(k, d, s + 1)
                        self.share(k, d, s)
            for k in self.ks:
                for d in (0, 1):
                    if s + d <= 4:
                        self.shared(k, d, s)
            for k in self.ks:
                for d in (0, 1):
                    if s + d <= 4:
                        work(k, self.back(k, d, s))
        for copy in self.pending:
            copy.wait_send()


def torus_sems(n):
    dma = pltpu.SemaphoreType.DMA
    return [dma((n, 7)), dma((n, 7)), dma((n, 2, 4)), dma((n, 2, 4)), dma((n, 2, 5)), dma((n, 2, 5))]


def meet(devices):
    barrier = pltpu.get_barrier_semaphore()
    for device in devices:
        pl.semaphore_signal(barrier, inc=1, device_id=device, device_id_type=MESH)
    pl.semaphore_wait(barrier, len(devices))


def params(collective_id=None):
    more = {} if collective_id is None else {"collective_id": collective_id, "has_side_effects": True}
    return pltpu.CompilerParams(vmem_limit_bytes=60 * 1024 * 1024, **more)


def index_of(z, y, c):
    return (z * RING + y) * 2 + c


def coords_of(index):
    return {"sp_0": index // 16, "sp_1": lax.rem(index // 2, RING), "sp_2": lax.rem(index, 2)}


def project_kernel(x_ref, gain_ref, w_ref, oa_ref, ob_ref, ga, gb, halo, normed, hs, hr, *sems):
    cut, width = ga.shape[-1], w_ref.shape[-1]
    torus = Torus([(w_ref.at[:, pl.ds(0, cut)], ga, "y"), (w_ref.at[:, pl.ds(cut, width - cut)], gb, "z")], sems)
    me = index_of(torus.z, torus.y, torus.c)
    later, earlier = coords_of(lax.rem(me + 1, 128)), coords_of(lax.rem(me + 127, 128))
    meet(torus.peers() + [later, earlier])
    span = x_ref.shape[1]
    torus.go(x_ref.at[:, pl.ds(span - HALO, HALO)], halo, hs, hr, later)
    torus.begin()
    rows = span + HALO

    def norm(values):
        wide = values.astype(F32)
        scale = lax.rsqrt(jnp.mean(wide * wide, axis=-1, keepdims=True) + EPS)
        return (wide * scale * gain_ref[...]).astype(BF16)

    for b in range(2):
        for r in range(0, span, 32):
            normed[b * rows + HALO + r:b * rows + HALO + r + 32] = norm(x_ref[b, r:r + 32])
    torus.arrived(halo, hs, hr)
    for b in range(2):
        normed[b * rows:b * rows + HALO] = norm(halo[b])
    torus.finish()
    depth = normed.shape[1]
    for g, o in ((ga, oa_ref), (gb, ob_ref)):
        o[...] = jnp.dot(normed[...], g[...].reshape(depth, g.shape[-1]), preferred_element_type=F32)


def project(x, gain, w, cut):
    rows = 2 * (x.shape[1] + HALO)
    dma = pltpu.SemaphoreType.DMA
    return pl.pallas_call(
        project_kernel,
        out_shape=[jax.ShapeDtypeStruct((rows, n), F32) for n in (cut, w.shape[1] - cut)],
        in_specs=[VMEM] * 3,
        out_specs=[VMEM] * 2,
        scratch_shapes=[
            *[pltpu.VMEM((8, 8, 2, w.shape[0], n), BF16) for n in (cut, w.shape[1] - cut)],
            pltpu.VMEM((2, HALO, x.shape[2]), BF16),
            pltpu.VMEM((rows, x.shape[2]), BF16),
            dma,
            dma,
            *torus_sems(2),
        ],
        compiler_params=params(0),
    )(x, gain, w)


def head_scale(values, gain):
    return values * lax.rsqrt(jnp.mean(values * values, axis=-1, keepdims=True) + EPS) * gain


def softplus(values):
    grown = jnp.exp(-jnp.abs(values))
    series = jnp.zeros_like(grown)
    for n in range(8, 0, -1):
        series = grown * ((1.0 if n % 2 else -1.0) / n + series)
    return jnp.maximum(values, 0.0) + jnp.where(grown < 0.06, series, jnp.log(1.0 + grown))


def one_less_exp(values):
    series = jnp.zeros_like(values)
    for n in range(8, 0, -1):
        series = values / n * (1.0 + series)
    return jnp.where(values > -0.3, -series, 1.0 - jnp.exp(values))


def local_kernel(
    oa_ref, ob_ref, qg_ref, kg_ref, cw_ref, dw_ref, iw_ref, dp_ref, de_ref, q_ref, k0_ref, k1_ref, cum_ref, loc_ref, sum_ref
):
    span = q_ref.shape[1] // 4
    rows = span + HALO
    me = lax.axis_index(SP)
    lane = lax.broadcasted_iota(jnp.int32, (span, 16), 1)
    power = softplus(-dp_ref[...]) * -8.0
    for b, k_ref in enumerate((k0_ref, k1_ref)):
        own = pl.ds(b * rows + HALO, span)
        proj = oa_ref[own, :256]
        for h in range(4):
            q = head_scale(proj[:, h * 64:(h + 1) * 64], qg_ref[...]).astype(BF16).astype(F32) * 0.125
            picks = jnp.where((lane % 4 == h) & (lane < 12), 1.0, 0.0)
            q_ref[b, h * span:(h + 1) * span] = jnp.concatenate([q, picks], axis=1).astype(BF16)
        kv = ob_ref[own, :128]
        key = head_scale(kv[:, :64], kg_ref[...])
        k_ref[...] = jnp.concatenate([key, kv[:, 64:]], axis=1).T.astype(BF16)
        before = oa_ref[b * rows:b * rows + HALO, 256:] * jnp.where(me > 0, 1.0, 0.0)
        ext = jnp.concatenate([before, oa_ref[own, 256:]], axis=0).astype(BF16).astype(F32)
        conv = jnp.zeros((span, 256), F32)
        for k in range(4):
            conv = conv + ext[HALO - 3 + k:HALO - 3 + k + span] * cw_ref[k:k + 1].astype(F32)
        conv = conv.astype(BF16)
        gd, gi = (
            jnp.concatenate(
                [jnp.dot(conv[:, n * 64:(n + 1) * 64], w[n], preferred_element_type=F32) for n in range(4)], axis=1
            )
            for w in (dw_ref, iw_ref)
        )
        log_decay = power * jax.nn.sigmoid(gd) + de_ref[b]
        add = jnp.sqrt(one_less_exp(2.0 * log_decay)) * jax.nn.sigmoid(gi) * conv.astype(F32)
        mul = jnp.exp(log_decay)
        s = 1
        while s < span:
            mul_b = jnp.concatenate([jnp.ones((s, 256), F32), mul[:-s]], axis=0)
            add_b = jnp.concatenate([jnp.zeros((s, 256), F32), add[:-s]], axis=0)
            add = mul * add_b + add
            mul = mul * mul_b
            s *= 2
        cum_ref[b] = mul
        loc_ref[b] = add
        sum_ref[0, b:b + 1] = mul[span - 1:]
        sum_ref[1, b:b + 1] = add[span - 1:]


def local(oa, ob, *more):
    span = oa.shape[0] // 2 - HALO
    shape = jax.ShapeDtypeStruct
    return pl.pallas_call(
        local_kernel,
        out_shape=[
            shape((2, 4 * span, 80), BF16),
            *[shape((128, span), BF16)] * 2,
            *[shape((2, span, 256), F32)] * 2,
            shape((2, 2, 256), F32),
        ],
        in_specs=[VMEM] * 9,
        out_specs=[VMEM] * 6,
        compiler_params=params(),
    )(oa, ob, *more)


def gate_pieces(rel):
    hi = rel.astype(BF16).astype(F32)
    mid = (rel - hi).astype(BF16).astype(F32)
    return jnp.concatenate([hi, mid, rel - hi - mid, jnp.zeros_like(rel)], axis=0).astype(BF16)


def mix_kernel(
    k0_ref, k1_ref, ends_ref, q_ref, forget_ref, ag_ref, cum_ref, loc_ref, ob_ref, rg_ref, wa_ref, wr_ref, out_ref,
    kv0, kv1, st, gates, acc, top, normed, terms, held, send, recv, *sems
):
    seqs, rows, depth = q_ref.shape
    span = k0_ref.shape[1]
    heads = rows // span
    torus = Torus([(k0_ref, kv0, "y"), (k1_ref, kv1, "z"), (ends_ref, st, "y")], sems)
    column = lax.axis_index("tp")
    peers = [lax.rem(column + j, 4) for j in range(4)]
    meet(torus.peers() + [{"tp": p} for p in peers[1:]])
    torus.begin()
    me = index_of(torus.z, torus.y, torus.c)
    first = pl.multiple_of(me * span, span)
    line = 16 * span
    ones_own = jnp.ones((16, span), BF16)
    ones = jnp.ones((16, line), BF16)
    row = lax.broadcasted_iota(jnp.int32, (rows, span), 0) % span
    col = lax.broadcasted_iota(jnp.int32, (rows, span), 1)
    for b, k_ref in enumerate((k0_ref, k1_ref)):
        near = forget_ref[b, :, pl.ds(first, span)]
        base = near[:, :1]

        def prep(c, _):
            at = pl.multiple_of(c * line, line)
            rel = base - forget_ref[b, :, pl.ds(at, line)]
            pos = at + lax.broadcasted_iota(jnp.int32, rel.shape, 1)
            gates[b, :, pl.ds(at, line)] = gate_pieces(jnp.where(pos < first, rel, -1e30))
            return 0

        lax.fori_loop(0, RING, prep, 0)
        own = k_ref[...]
        rhs = jnp.concatenate([own[:64], gate_pieces(base - near)], axis=0)
        s = jnp.dot(q_ref[b], rhs, preferred_element_type=F32)
        s = jnp.where(row >= col, s, -jnp.inf)
        m = jnp.max(s, axis=1, keepdims=True)
        p = jnp.exp(s - m).astype(BF16)
        acc[b] = lax.dot_general(p, jnp.concatenate([own[64:], ones_own], axis=0), NT, preferred_element_type=F32)
        top[b] = jnp.broadcast_to(m, (rows, 128))

    def attend(b, blocks, near_gates):
        rhs = jnp.concatenate([jnp.concatenate([x[:64] for x in blocks], axis=1), near_gates], axis=0)
        s = jnp.dot(q_ref[b], rhs, preferred_element_type=F32)
        old = top[b][:, :1]
        m = jnp.maximum(old, jnp.max(s, axis=1, keepdims=True))
        p = jnp.exp(s - m).astype(BF16)
        vx = jnp.concatenate([jnp.concatenate([x[64:] for x in blocks], axis=1), ones], axis=0)
        acc[b] = acc[b] * jnp.exp(old - m) + lax.dot_general(p, vx, NT, preferred_element_type=F32)
        top[b] = jnp.broadcast_to(m, (rows, 128))

    def work(k, j):
        if k == 0:
            @pl.when(j * 16 < me)
            def _():
                attend(0, [kv0[j, i // 2, i % 2] for i in range(16)], gates[0, :, pl.ds(pl.multiple_of(j * line, line), line)])
        if k == 1:
            @pl.when(j * 2 < me)
            def _():
                parts = [gates[1, :, pl.ds(pl.multiple_of((z * RING + j) * 2 * span, 2 * span), 2 * span)] for z in range(RING)]
                attend(1, [kv1[i // 2, j, i % 2] for i in range(16)], jnp.concatenate(parts, axis=1))

    torus.finish(work)

    def merge(j, state):
        part = st.at[j // 16, lax.rem(j // 2, RING), lax.rem(j, 2)]
        return part[0] * state + part[1]

    entering = lax.fori_loop(0, me, merge, jnp.zeros((2, 256), F32))
    wide_rows = span + HALO
    for b in range(seqs):
        a = acc[b]
        att = head_scale(a[:, :64] / a[:, 64:65], 1.0)
        att = jnp.concatenate([att[h * span:(h + 1) * span] for h in range(heads)], axis=1)
        normed[0, b * span:(b + 1) * span] = (att * ag_ref[...]).astype(BF16)
        state = loc_ref[b] + cum_ref[b] * entering[b:b + 1]
        gated = state * jax.nn.gelu(ob_ref[pl.ds(b * wide_rows + HALO, span), 128:])
        rec = jnp.concatenate([head_scale(gated[:, n * 64:(n + 1) * 64], 1.0) for n in range(4)], axis=1)
        normed[1, b * span:(b + 1) * span] = (rec * rg_ref[...]).astype(BF16)
    width = out_ref.shape[1]
    copies = []
    for j in (2, 1, 3, 0):
        part = pl.ds(pl.multiple_of(peers[j] * width, width), width)
        total = jnp.dot(normed[0], wa_ref[:, part], preferred_element_type=F32)
        total = total + jnp.dot(normed[1], wr_ref[:, part], preferred_element_type=F32)
        terms[j] = total.astype(BF16)
        if j:
            copy = pltpu.make_async_remote_copy(
                src_ref=terms.at[j], dst_ref=held.at[j - 1], send_sem=send.at[j - 1], recv_sem=recv.at[j - 1],
                device_id={"tp": peers[j]}, device_id_type=MESH,
            )
            copy.start()
            copies.append(copy)
    for copy in copies:
        copy.wait()
    total = terms[0].astype(F32)
    for j in range(3):
        total = total + held[j].astype(F32)
    out_ref[...] = total.astype(BF16)


def mix(k0, k1, ends, q, forget, *more):
    span, length = k0.shape[1], forget.shape[2]
    rows = q.shape[1]
    width = more[-1].shape[1] // 4
    dma = pltpu.SemaphoreType.DMA
    return pl.pallas_call(
        mix_kernel,
        out_shape=jax.ShapeDtypeStruct((2 * span, width), BF16),
        in_specs=[VMEM] * (5 + len(more)),
        out_specs=VMEM,
        scratch_shapes=[
            pltpu.VMEM((8, 8, 2, *k0.shape), BF16),
            pltpu.VMEM((8, 8, 2, *k1.shape), BF16),
            pltpu.VMEM((8, 8, 2, *ends.shape), F32),
            pltpu.VMEM((2, 16, length), BF16),
            pltpu.VMEM((2, rows, 80), F32),
            pltpu.VMEM((2, rows, 128), F32),
            pltpu.VMEM((2, 2 * span, 256), BF16),
            pltpu.VMEM((4, 2 * span, width), BF16),
            pltpu.VMEM((3, 2 * span, width), BF16),
            dma((3,)),
            dma((3,)),
            *torus_sems(3),
        ],
        compiler_params=params(1),
    )(k0, k1, ends, q, forget, *more)


def body(
    inputs, norm_gain, query_weight, key_weight, value_weight, query_gain, key_gain, forget_cache, rec_in_weight,
    rec_gate_weight, conv_weight, decay_gate_weight, input_gate_weight, decay_param, decay_extra, attn_out_gain,
    rec_out_gain, out_att_weight, out_rec_weight,
):
    span = inputs.shape[1]
    cut = query_weight.shape[1] + rec_in_weight.shape[1]
    joined = jnp.concatenate([query_weight, rec_in_weight, key_weight, value_weight, rec_gate_weight], axis=1)
    oa, ob = project(inputs, norm_gain[None], joined, cut)
    q, k0, k1, cum, loc, ends = local(
        oa, ob, query_gain[None], key_gain[None], conv_weight, decay_gate_weight, input_gate_weight, decay_param[None],
        decay_extra,
    )
    mixed = mix(
        k0, k1, ends, q, forget_cache, attn_out_gain[None], cum, loc, ob, rec_out_gain[None], out_att_weight,
        out_rec_weight,
    )
    return mixed.reshape(2, span, -1)


def solution(mesh):
    finer = Mesh(mesh.devices.reshape(8, 8, 2, mesh.shape["tp"]), (*SP, "tp"))
    return jax.shard_map(
        body,
        mesh=finer,
        in_specs=(
            P(None, SP, None), P(), P(SP, "tp"), P(SP, "tp"), P(SP, "tp"), P(), P(), P(None, "tp", None), P(SP, "tp"),
            P(SP, "tp"), P(None, "tp"), P("tp", None, None), P("tp", None, None), P("tp"), P(None, SP, "tp"), P("tp"),
            P("tp"), P("tp", None), P("tp", None),
        ),
        out_specs=P(None, SP, "tp"),
        check_vma=False,
    )
```

```python
import functools

import jax
import jax.numpy as jnp
from jax import lax
from jax.experimental import pallas as pl
from jax.experimental.pallas import tpu as pltpu
from jax.sharding import Mesh
from jax.sharding import PartitionSpec as P

SP = ("sp_0", "sp_1", "sp_2")
NT = (((1,), (1,)), ((), ()))
EPS = 1e-6
HALO = 16
F32, BF16 = jnp.float32, jnp.bfloat16
VMEM = pl.BlockSpec(memory_space=pltpu.VMEM)

MESH = pl.DeviceIdType.MESH
RING = 8


class Torus:
    def __init__(self, streams, sems):
        self.streams = streams
        self.s1, self.r1, self.s2, self.r2, self.ps, self.pr = sems
        self.z, self.y, self.c = (lax.axis_index(n) for n in SP)
        self.sign = 1 - 2 * self.c
        self.other = {"sp_2": 1 - self.c}
        self.ks = range(len(streams))

    def peers(self):
        found = [self.other]
        for name, pos in (("sp_0", self.z), ("sp_1", self.y)):
            found += [{name: lax.rem(pos + i, RING)} for i in range(1, RING)]
        return found

    def places(self, k):
        return (self.y, self.z) if self.streams[k][2] == "y" else (self.z, self.y)

    def axes(self, k):
        return ("sp_1", "sp_0") if self.streams[k][2] == "y" else ("sp_0", "sp_1")

    def one(self, k, i):
        o, first = self.streams[k][1:]
        return o.at[self.z, i, self.c] if first == "y" else o.at[i, self.y, self.c]

    def line(self, k, j, core):
        o, first = self.streams[k][1:]
        return o.at[j, :, core] if first == "y" else o.at[:, j, core]

    def back(self, k, d, s):
        sg = self.sign if d == 0 else -self.sign
        return lax.rem(self.places(k)[1] - sg * s + RING, RING)

    def copy(self, src, dst, send, recv, device):
        return pltpu.make_async_remote_copy(
            src_ref=src, dst_ref=dst, send_sem=send, recv_sem=recv, device_id=device, device_id_type=MESH
        )

    def arrived(self, ref, send, recv):
        self.copy(ref, ref, send, recv, self.other).wait_recv()

    def begin(self):
        for i in (4, 5, 3, 6, 2, 7, 1):
            for k in self.ks:
                pos = self.places(k)[0]
                self.copy(
                    self.streams[k][0], self.one(k, pos), self.s1.at[k, i - 1], self.r1.at[k, i - 1],
                    {self.axes(k)[0]: lax.rem(pos + i, RING)},
                ).start()
        for k in self.ks:
            self.streams[k][1][self.z, self.y, self.c] = self.streams[k][0][...]

    def joined(self, k):
        pos = self.places(k)[0]
        for i in range(1, RING):
            got = self.one(k, lax.rem(pos + RING - i, RING))
            self.arrived(got, self.s1.at[k, i - 1], self.r1.at[k, i - 1])

    def pass_on(self, k, d, s):
        ref = self.line(k, self.back(k, d, s - 1), self.c)
        device = {self.axes(k)[1]: self.back(k, d, -1)}
        self.copy(ref, ref, self.s2.at[k, d, s - 1], self.r2.at[k, d, s - 1], device).start()

    def share(self, k, j, d, s):
        ref = self.line(k, j, self.c)
        self.copy(ref, ref, self.ps.at[k, d, s], self.pr.at[k, d, s], self.other).start()

    def shared(self, k, j, d, s):
        self.arrived(self.line(k, j, 1 - self.c), self.ps.at[k, d, s], self.pr.at[k, d, s])

    def lines(self):
        for k in self.ks:
            self.joined(k)
            for d in (0, 1):
                self.pass_on(k, d, 1)
            self.share(k, self.places(k)[1], 0, 0)

    def step(self, s):
        for k in self.ks:
            for d in (0, 1):
                if not isinstance(s, int) or s + d <= 4:
                    got = self.line(k, self.back(k, d, s), self.c)
                    self.arrived(got, self.s2.at[k, d, s - 1], self.r2.at[k, d, s - 1])
                    if isinstance(s, int):
                        if s + d < 4:
                            self.pass_on(k, d, s + 1)
                    else:
                        pl.when(s + d < 4)(functools.partial(self.pass_on, k, d, s + 1))
                    self.share(k, self.back(k, d, s), d, s)

    def step_shared(self, s):
        for k in self.ks:
            for d in (0, 1):
                if not isinstance(s, int) or s + d <= 4:
                    self.shared(k, self.back(k, d, -s), d, s)

    def own_shared(self):
        for k in self.ks:
            self.shared(k, self.places(k)[1], 0, 0)

    def drain(self):
        for k in self.ks:
            one, line = self.streams[k][0], self.line(k, self.places(k)[1], self.c)
            for i in range(7):
                self.copy(one, one, self.s1.at[k, i], self.r1.at[k, i], self.other).wait_send()
            self.copy(line, line, self.ps.at[k, 0, 0], self.pr.at[k, 0, 0], self.other).wait_send()
            for i in range(7):
                d, s = i // 4, i % 4
                self.copy(line, line, self.s2.at[k, d, s], self.r2.at[k, d, s], self.other).wait_send()
                self.copy(line, line, self.ps.at[k, d, s + 1], self.pr.at[k, d, s + 1], self.other).wait_send()

    def short_lines(self):
        for k in self.ks:
            self.joined(k)
            pos = self.places(k)[1]
            ref = self.line(k, pos, self.c)
            for i in (4, 5, 3, 6, 2, 7, 1):
                d, s = (i - 1) // 4, (i - 1) % 4
                device = {self.axes(k)[1]: lax.rem(pos + i, RING)}
                self.copy(ref, ref, self.s2.at[k, d, s], self.r2.at[k, d, s], device).start()
            self.share(k, pos, 0, 0)

    def short_finish(self):
        for k in self.ks:
            pos = self.places(k)[1]
            for i in (1, 7, 2, 6, 3, 5, 4):
                d, s = (i - 1) // 4, (i - 1) % 4
                j = lax.rem(pos + RING - i, RING)
                self.arrived(self.line(k, j, self.c), self.s2.at[k, d, s], self.r2.at[k, d, s])
                self.share(k, j, d, s + 1)
            self.shared(k, pos, 0, 0)
            for i in range(1, RING):
                self.shared(k, lax.rem(pos + RING - i, RING), (i - 1) // 4, (i - 1) % 4 + 1)


def torus_sems(n):
    dma = pltpu.SemaphoreType.DMA
    return [dma((n, 7)), dma((n, 7)), dma((n, 2, 4)), dma((n, 2, 4)), dma((n, 2, 5)), dma((n, 2, 5))]


def meet(devices):
    barrier = pltpu.get_barrier_semaphore()
    for device in devices:
        pl.semaphore_signal(barrier, inc=1, device_id=device, device_id_type=MESH)
    pl.semaphore_wait(barrier, len(devices))

def params(collective_id=None):
    more = {} if collective_id is None else {"collective_id": collective_id, "has_side_effects": True}
    return pltpu.CompilerParams(vmem_limit_bytes=60 * 1024 * 1024, **more)


def index_of(z, y, c):
    return (z * RING + y) * 2 + c


def coords_of(index):
    return {"sp_0": index // 16, "sp_1": lax.rem(index // 2, RING), "sp_2": lax.rem(index, 2)}


def head_scale(values, gain):
    return values * lax.rsqrt(jnp.mean(values * values, axis=-1, keepdims=True) + EPS) * gain


def softplus(values):
    grown = jnp.exp(-jnp.abs(values))
    series = jnp.zeros_like(grown)
    for n in range(8, 0, -1):
        series = grown * ((1.0 if n % 2 else -1.0) / n + series)
    return jnp.maximum(values, 0.0) + jnp.where(grown < 0.06, series, jnp.log(1.0 + grown))


def one_less_exp(values):
    series = jnp.zeros_like(values)
    for n in range(8, 0, -1):
        series = values / n * (1.0 + series)
    return jnp.where(values > -0.3, -series, 1.0 - jnp.exp(values))


def gate_pieces(rel):
    hi = rel.astype(BF16).astype(F32)
    mid = (rel - hi).astype(BF16).astype(F32)
    return jnp.concatenate([hi, mid, rel - hi - mid, jnp.zeros_like(rel)], axis=0).astype(BF16)


def kernel(
    x_ref, gain_ref, w_ref, qg_ref, kg_ref, cw_ref, dw_ref, iw_ref, dp_ref, de_ref, forget_ref, ag_ref, rg_ref, wa_ref,
    wr_ref, out_ref, gk, ga, gb, kv0, kv1, st, halo, normed, proj, k0_ref, k1_ref, ends, q_ref, gates, acc, top, cum, loc,
    mixed, terms, held, send, recv, hs, hr, *sems
):
    seqs, rows, depth = q_ref.shape
    span = k0_ref.shape[1]
    heads = rows // span
    wide = span + HALO
    ck, ca, cb = gk.shape[-1], ga.shape[-1], gb.shape[-1]
    first_w = Torus([(w_ref.at[:, pl.ds(0, ck)], gk, "y")], sems[:6])
    more_w = Torus([(w_ref.at[:, pl.ds(ck, ca)], ga, "y"), (w_ref.at[:, pl.ds(ck + ca, cb)], gb, "z")], sems[6:12])
    keys = Torus([(k0_ref, kv0, "y"), (k1_ref, kv1, "z")], sems[12:18])
    chain = Torus([(ends, st, "y")], sems[18:])
    me = index_of(keys.z, keys.y, keys.c)
    later, earlier = coords_of(lax.rem(me + 1, 128)), coords_of(lax.rem(me + 127, 128))
    column = lax.axis_index("tp")
    peers = [lax.rem(column + j, 4) for j in range(4)]
    meet(keys.peers() + [{"tp": p} for p in peers[1:]] + [later, earlier])
    first_w.begin()
    edge = keys.copy(x_ref.at[:, pl.ds(span - HALO, HALO)], halo, hs, hr, later)
    edge.start()
    more_w.begin()

    def norm(values):
        full = values.astype(F32)
        scale = lax.rsqrt(jnp.mean(full * full, axis=-1, keepdims=True) + EPS)
        return (full * scale * gain_ref[...]).astype(BF16)

    for b in range(seqs):
        for r in range(0, span, 32):
            normed[b * wide + HALO + r:b * wide + HALO + r + 32] = norm(x_ref[b, r:r + 32])
    first_w.short_lines()
    edge.wait()
    for b in range(seqs):
        normed[b * wide:b * wide + HALO] = norm(halo[b])
    more_w.lines()
    more_w.step(1)
    first_w.short_finish()
    kv_proj = jnp.dot(normed[...], gk[...].reshape(-1, ck), preferred_element_type=F32)
    for b, k_ref in enumerate((k0_ref, k1_ref)):
        kv = kv_proj[b * wide + HALO:(b + 1) * wide]
        k_ref[...] = jnp.concatenate([head_scale(kv[:, :64], kg_ref[...]), kv[:, 64:]], axis=1).T.astype(BF16)
    keys.begin()
    more_w.step(2)

    first = pl.multiple_of(me * span, span)
    line = 16 * span
    for b in range(seqs):
        base = forget_ref[b, :, pl.ds(first, span)][:, :1]

        def prep(c, _):
            at = pl.multiple_of(c * line, line)
            rel = base - forget_ref[b, :, pl.ds(at, line)]
            pos = at + lax.broadcasted_iota(jnp.int32, rel.shape, 1)
            gates[b, :, pl.ds(at, line)] = gate_pieces(jnp.where(pos < first, rel, -1e30))
            return 0

        lax.fori_loop(0, RING, prep, 0)
    more_w.step(3)
    keys.lines()
    more_w.step(4)
    more_w.own_shared()
    for s in range(1, 5):
        more_w.step_shared(s)
    for g, at, n in ((ga, 0, ca), (gb, ca, cb)):
        proj[:, at:at + n] = jnp.dot(normed[...], g[...].reshape(-1, n), preferred_element_type=F32)

    power = softplus(-dp_ref[...]) * -8.0
    for b in range(seqs):
        own = pl.ds(b * wide + HALO, span)
        before = proj[b * wide:b * wide + HALO, 256:512] * jnp.where(me > 0, 1.0, 0.0)
        ext = jnp.concatenate([before, proj[own, 256:512]], axis=0).astype(BF16).astype(F32)
        conv = jnp.zeros((span, 256), F32)
        for k in range(4):
            conv = conv + ext[HALO - 3 + k:HALO - 3 + k + span] * cw_ref[k:k + 1].astype(F32)
        conv = conv.astype(BF16)
        gd, gi = (
            jnp.concatenate(
                [jnp.dot(conv[:, n * 64:(n + 1) * 64], w[n], preferred_element_type=F32) for n in range(4)], axis=1
            )
            for w in (dw_ref, iw_ref)
        )
        log_decay = power * jax.nn.sigmoid(gd) + de_ref[b]
        add = jnp.sqrt(one_less_exp(2.0 * log_decay)) * jax.nn.sigmoid(gi) * conv.astype(F32)
        mul = jnp.exp(log_decay)
        s = 1
        while s < span:
            mul_b = jnp.concatenate([jnp.ones((s, 256), F32), mul[:-s]], axis=0)
            add_b = jnp.concatenate([jnp.zeros((s, 256), F32), add[:-s]], axis=0)
            add = mul * add_b + add
            mul = mul * mul_b
            s *= 2
        cum[b] = mul
        loc[b] = add
        ends[0, b:b + 1] = mul[span - 1:]
        ends[1, b:b + 1] = add[span - 1:]
    chain.begin()

    ones_own = jnp.ones((16, span), BF16)
    ones = jnp.ones((16, line), BF16)
    row = lax.broadcasted_iota(jnp.int32, (rows, span), 0) % span
    col = lax.broadcasted_iota(jnp.int32, (rows, span), 1)
    lane = lax.broadcasted_iota(jnp.int32, (span, 16), 1)
    for b, k_ref in enumerate((k0_ref, k1_ref)):
        query = proj[pl.ds(b * wide + HALO, span), :256]
        for h in range(heads):
            q = head_scale(query[:, h * 64:(h + 1) * 64], qg_ref[...]).astype(BF16).astype(F32) * 0.125
            picks = jnp.where((lane % 4 == h) & (lane < 12), 1.0, 0.0)
            q_ref[b, h * span:(h + 1) * span] = jnp.concatenate([q, picks], axis=1).astype(BF16)
        near = forget_ref[b, :, pl.ds(first, span)]
        own = k_ref[...]
        rhs = jnp.concatenate([own[:64], gate_pieces(near[:, :1] - near)], axis=0)
        s = jnp.dot(q_ref[b], rhs, preferred_element_type=F32)
        s = jnp.where(row >= col, s, -jnp.inf)
        m = jnp.max(s, axis=1, keepdims=True)
        p = jnp.exp(s - m).astype(BF16)
        acc[b] = lax.dot_general(p, jnp.concatenate([own[64:], ones_own], axis=0), NT, preferred_element_type=F32)
        top[b] = jnp.broadcast_to(m, (rows, 128))

    def attend(b, blocks, near_gates):
        rhs = jnp.concatenate([jnp.concatenate([x[:64] for x in blocks], axis=1), near_gates], axis=0)
        s = jnp.dot(q_ref[b], rhs, preferred_element_type=F32)
        old = top[b][:, :1]
        m = jnp.maximum(old, jnp.max(s, axis=1, keepdims=True))
        p = jnp.exp(s - m).astype(BF16)
        vx = jnp.concatenate([jnp.concatenate([x[64:] for x in blocks], axis=1), ones], axis=0)
        acc[b] = acc[b] * jnp.exp(old - m) + lax.dot_general(p, vx, NT, preferred_element_type=F32)
        top[b] = jnp.broadcast_to(m, (rows, 128))

    def work_0(j):
        @pl.when(j * 16 < me)
        def _():
            attend(0, [kv0[j, i // 2, i % 2] for i in range(16)], gates[0, :, pl.ds(pl.multiple_of(j * line, line), line)])

    def work_1(j):
        @pl.when(j * 2 < me)
        def _():
            parts = [gates[1, :, pl.ds(pl.multiple_of((z * RING + j) * 2 * span, 2 * span), 2 * span)] for z in range(RING)]
            attend(1, [kv1[i // 2, j, i % 2] for i in range(16)], jnp.concatenate(parts, axis=1))

    keys.step(1)
    keys.own_shared()
    work_0(keys.z)
    work_1(keys.y)
    chain.lines()

    for s in range(1, 4):
        keys.step_shared(s)

        def both(d, _):
            sg = keys.sign * (1 - 2 * d)
            work_0(lax.rem(keys.z - sg * s + RING, RING))
            work_1(lax.rem(keys.y - sg * s + RING, RING))
            return 0

        lax.fori_loop(0, 2, both, 0)
        keys.step(s + 1)
        chain.step(s)
    keys.step_shared(4)
    work_0(keys.back(0, 0, 4))
    work_1(keys.back(1, 0, 4))
    chain.step(4)
    chain.own_shared()
    for s in range(1, 5):
        chain.step_shared(s)

    def merge(j, state):
        part = st.at[j // 16, lax.rem(j // 2, RING), lax.rem(j, 2)]
        return part[0] * state + part[1]

    entering = lax.fori_loop(0, me, merge, jnp.zeros((2, 256), F32))
    for b in range(seqs):
        a = acc[b]
        att = head_scale(a[:, :64] / a[:, 64:65], 1.0)
        att = jnp.concatenate([att[h * span:(h + 1) * span] for h in range(heads)], axis=1)
        mixed[0, b * span:(b + 1) * span] = (att * ag_ref[...]).astype(BF16)
        state = loc[b] + cum[b] * entering[b:b + 1]
        gated = state * jax.nn.gelu(proj[pl.ds(b * wide + HALO, span), 512:])
        rec = jnp.concatenate([head_scale(gated[:, n * 64:(n + 1) * 64], 1.0) for n in range(4)], axis=1)
        mixed[1, b * span:(b + 1) * span] = (rec * rg_ref[...]).astype(BF16)
    width = out_ref.shape[1]
    copies = []
    for j in (2, 1, 3, 0):
        part = pl.ds(pl.multiple_of(peers[j] * width, width), width)
        total = jnp.dot(mixed[0], wa_ref[:, part], preferred_element_type=F32)
        total = total + jnp.dot(mixed[1], wr_ref[:, part], preferred_element_type=F32)
        terms[j] = total.astype(BF16)
        if j:
            copy = keys.copy(terms.at[j], held.at[j - 1], send.at[j - 1], recv.at[j - 1], {"tp": peers[j]})
            copy.start()
            copies.append(copy)
    for group in (first_w, more_w, keys, chain):
        group.drain()
    for copy in copies:
        copy.wait()
    total = terms[0].astype(F32)
    for j in range(3):
        total = total + held[j].astype(F32)
    out_ref[...] = total.astype(BF16)


def layer(x, gain, w, *more):
    span, length, out_cols = x.shape[1], more[7].shape[2], more[-1].shape[1]
    wide, width = 2 * (span + HALO), out_cols // 4
    dma = pltpu.SemaphoreType.DMA

    def grid(dtype, *shape):
        return pltpu.VMEM((8, 8, 2, *shape), dtype)

    return pl.pallas_call(
        kernel,
        out_shape=jax.ShapeDtypeStruct((2 * span, width), BF16),
        in_specs=[VMEM] * (3 + len(more)),
        out_specs=VMEM,
        scratch_shapes=[
            grid(BF16, w.shape[0], 128),
            grid(BF16, w.shape[0], 384),
            grid(BF16, w.shape[0], 384),
            grid(BF16, 128, span),
            grid(BF16, 128, span),
            grid(F32, 2, 2, 256),
            pltpu.VMEM((2, HALO, x.shape[2]), BF16),
            pltpu.VMEM((wide, x.shape[2]), BF16),
            pltpu.VMEM((wide, 768), F32),
            pltpu.VMEM((128, span), BF16),
            pltpu.VMEM((128, span), BF16),
            pltpu.VMEM((2, 2, 256), F32),
            pltpu.VMEM((2, 4 * span, 80), BF16),
            pltpu.VMEM((2, 16, length), BF16),
            pltpu.VMEM((2, 4 * span, 80), F32),
            pltpu.VMEM((2, 4 * span, 128), F32),
            pltpu.VMEM((2, span, 256), F32),
            pltpu.VMEM((2, span, 256), F32),
            pltpu.VMEM((2, 2 * span, 256), BF16),
            pltpu.VMEM((4, 2 * span, width), BF16),
            pltpu.VMEM((3, 2 * span, width), BF16),
            dma((3,)),
            dma((3,)),
            dma,
            dma,
            *torus_sems(1),
            *torus_sems(2),
            *torus_sems(2),
            *torus_sems(1),
        ],
        compiler_params=params(0),
    )(x, gain, w, *more)


def body(
    inputs, norm_gain, query_weight, key_weight, value_weight, query_gain, key_gain, forget_cache, rec_in_weight,
    rec_gate_weight, conv_weight, decay_gate_weight, input_gate_weight, decay_param, decay_extra, attn_out_gain,
    rec_out_gain, out_att_weight, out_rec_weight,
):
    joined = jnp.concatenate([key_weight, value_weight, query_weight, rec_in_weight, rec_gate_weight], axis=1)
    mixed = layer(
        inputs, norm_gain[None], joined, query_gain[None], key_gain[None], conv_weight, decay_gate_weight,
        input_gate_weight, decay_param[None], decay_extra, forget_cache, attn_out_gain[None], rec_out_gain[None],
        out_att_weight, out_rec_weight,
    )
    return mixed.reshape(2, inputs.shape[1], -1)


def solution(mesh):
    finer = Mesh(mesh.devices.reshape(8, 8, 2, mesh.shape["tp"]), (*SP, "tp"))
    return jax.shard_map(
        body,
        mesh=finer,
        in_specs=(
            P(None, SP, None), P(), P(SP, "tp"), P(SP, "tp"), P(SP, "tp"), P(), P(), P(None, "tp", None), P(SP, "tp"),
            P(SP, "tp"), P(None, "tp"), P("tp", None, None), P("tp", None, None), P("tp"), P(None, SP, "tp"), P("tp"),
            P("tp"), P("tp", None), P("tp", None),
        ),
        out_specs=P(None, SP, "tp"),
        check_vma=False,
    )
```

```python
import functools

import jax
import jax.numpy as jnp
from jax import lax
from jax.experimental import pallas as pl
from jax.experimental.pallas import tpu as pltpu
from jax.sharding import Mesh
from jax.sharding import PartitionSpec as P

SP = ("sp_0", "sp_1", "sp_2")
NT = (((1,), (1,)), ((), ()))
EPS = 1e-6
HALO = 16
F32, BF16 = jnp.float32, jnp.bfloat16
VMEM = pl.BlockSpec(memory_space=pltpu.VMEM)
ANY = pl.BlockSpec(memory_space=pl.ANY)

MESH = pl.DeviceIdType.MESH
RING = 8


class Torus:
    def __init__(self, streams, sems):
        self.streams = streams
        self.s1, self.r1, self.s2, self.r2, self.ps, self.pr = sems
        self.z, self.y, self.c = (lax.axis_index(n) for n in SP)
        self.sign = 1 - 2 * self.c
        self.other = {"sp_2": 1 - self.c}
        self.ks = range(len(streams))

    def peers(self):
        found = [self.other]
        for name, pos in (("sp_0", self.z), ("sp_1", self.y)):
            found += [{name: lax.rem(pos + i, RING)} for i in range(1, RING)]
        return found

    def places(self, k):
        return (self.y, self.z) if self.streams[k][2] == "y" else (self.z, self.y)

    def axes(self, k):
        return ("sp_1", "sp_0") if self.streams[k][2] == "y" else ("sp_0", "sp_1")

    def one(self, k, i):
        o, first = self.streams[k][1:]
        return o.at[self.z, i, self.c] if first == "y" else o.at[i, self.y, self.c]

    def line(self, k, j, core):
        o, first = self.streams[k][1:]
        return o.at[j, :, core] if first == "y" else o.at[:, j, core]

    def back(self, k, d, s):
        sg = self.sign if d == 0 else -self.sign
        return lax.rem(self.places(k)[1] - sg * s + RING, RING)

    def copy(self, src, dst, send, recv, device):
        return pltpu.make_async_remote_copy(
            src_ref=src, dst_ref=dst, send_sem=send, recv_sem=recv, device_id=device, device_id_type=MESH
        )

    def arrived(self, ref, send, recv):
        self.copy(ref, ref, send, recv, self.other).wait_recv()

    def begin(self):
        for i in (4, 5, 3, 6, 2, 7, 1):
            for k in self.ks:
                pos = self.places(k)[0]
                self.copy(
                    self.streams[k][0], self.one(k, pos), self.s1.at[k, i - 1], self.r1.at[k, i - 1],
                    {self.axes(k)[0]: lax.rem(pos + i, RING)},
                ).start()
        for k in self.ks:
            self.streams[k][1][self.z, self.y, self.c] = self.streams[k][0][...]

    def joined(self, k):
        pos = self.places(k)[0]
        for i in range(1, RING):
            got = self.one(k, lax.rem(pos + RING - i, RING))
            self.arrived(got, self.s1.at[k, i - 1], self.r1.at[k, i - 1])

    def pass_on(self, k, d, s):
        ref = self.line(k, self.back(k, d, s - 1), self.c)
        device = {self.axes(k)[1]: self.back(k, d, -1)}
        self.copy(ref, ref, self.s2.at[k, d, s - 1], self.r2.at[k, d, s - 1], device).start()

    def share(self, k, j, d, s):
        ref = self.line(k, j, self.c)
        self.copy(ref, ref, self.ps.at[k, d, s], self.pr.at[k, d, s], self.other).start()

    def shared(self, k, j, d, s):
        self.arrived(self.line(k, j, 1 - self.c), self.ps.at[k, d, s], self.pr.at[k, d, s])

    def lines(self):
        for k in self.ks:
            self.joined(k)
            for d in (0, 1):
                self.pass_on(k, d, 1)
            self.share(k, self.places(k)[1], 0, 0)

    def step(self, s):
        for k in self.ks:
            for d in (0, 1):
                if not isinstance(s, int) or s + d <= 4:
                    got = self.line(k, self.back(k, d, s), self.c)
                    self.arrived(got, self.s2.at[k, d, s - 1], self.r2.at[k, d, s - 1])
                    if isinstance(s, int):
                        if s + d < 4:
                            self.pass_on(k, d, s + 1)
                    else:
                        pl.when(s + d < 4)(functools.partial(self.pass_on, k, d, s + 1))
                    self.share(k, self.back(k, d, s), d, s)

    def step_shared(self, s):
        for k in self.ks:
            for d in (0, 1):
                if not isinstance(s, int) or s + d <= 4:
                    self.shared(k, self.back(k, d, -s), d, s)

    def own_shared(self):
        for k in self.ks:
            self.shared(k, self.places(k)[1], 0, 0)

    def drain(self):
        for k in self.ks:
            one, line = self.streams[k][0], self.line(k, self.places(k)[1], self.c)
            for i in range(7):
                self.copy(one, one, self.s1.at[k, i], self.r1.at[k, i], self.other).wait_send()
            self.copy(line, line, self.ps.at[k, 0, 0], self.pr.at[k, 0, 0], self.other).wait_send()
            for i in range(7):
                d, s = i // 4, i % 4
                self.copy(line, line, self.s2.at[k, d, s], self.r2.at[k, d, s], self.other).wait_send()
                self.copy(line, line, self.ps.at[k, d, s + 1], self.pr.at[k, d, s + 1], self.other).wait_send()

    def short_lines(self):
        for k in self.ks:
            self.joined(k)
            pos = self.places(k)[1]
            ref = self.line(k, pos, self.c)
            for i in (4, 5, 3, 6, 2, 7, 1):
                d, s = (i - 1) // 4, (i - 1) % 4
                device = {self.axes(k)[1]: lax.rem(pos + i, RING)}
                self.copy(ref, ref, self.s2.at[k, d, s], self.r2.at[k, d, s], device).start()
            self.share(k, pos, 0, 0)

    def short_finish(self):
        for k in self.ks:
            pos = self.places(k)[1]
            for i in (1, 7, 2, 6, 3, 5, 4):
                d, s = (i - 1) // 4, (i - 1) % 4
                j = lax.rem(pos + RING - i, RING)
                self.arrived(self.line(k, j, self.c), self.s2.at[k, d, s], self.r2.at[k, d, s])
                self.share(k, j, d, s + 1)
            self.shared(k, pos, 0, 0)
            for i in range(1, RING):
                self.shared(k, lax.rem(pos + RING - i, RING), (i - 1) // 4, (i - 1) % 4 + 1)


def torus_sems(n):
    dma = pltpu.SemaphoreType.DMA
    return [dma((n, 7)), dma((n, 7)), dma((n, 2, 4)), dma((n, 2, 4)), dma((n, 2, 5)), dma((n, 2, 5))]


def meet(devices):
    barrier = pltpu.get_barrier_semaphore()
    for device in devices:
        pl.semaphore_signal(barrier, inc=1, device_id=device, device_id_type=MESH)
    pl.semaphore_wait(barrier, len(devices))

def params(collective_id=None):
    more = {} if collective_id is None else {"collective_id": collective_id, "has_side_effects": True}
    return pltpu.CompilerParams(vmem_limit_bytes=60 * 1024 * 1024, **more)


def index_of(z, y, c):
    return (z * RING + y) * 2 + c


def coords_of(index):
    return {"sp_0": index // 16, "sp_1": lax.rem(index // 2, RING), "sp_2": lax.rem(index, 2)}


def head_scale(values, gain):
    return values * lax.rsqrt(jnp.mean(values * values, axis=-1, keepdims=True) + EPS) * gain


def softplus(values):
    grown = jnp.exp(-jnp.abs(values))
    series = jnp.zeros_like(grown)
    for n in range(8, 0, -1):
        series = grown * ((1.0 if n % 2 else -1.0) / n + series)
    return jnp.maximum(values, 0.0) + jnp.where(grown < 0.06, series, jnp.log(1.0 + grown))


def one_less_exp(values):
    series = jnp.zeros_like(values)
    for n in range(8, 0, -1):
        series = values / n * (1.0 + series)
    return jnp.where(values > -0.3, -series, 1.0 - jnp.exp(values))


def gate_pieces(rel):
    hi = rel.astype(BF16).astype(F32)
    mid = (rel - hi).astype(BF16).astype(F32)
    return jnp.concatenate([hi, mid, rel - hi - mid, jnp.zeros_like(rel)], axis=0).astype(BF16)


def kernel(
    x_ref, gain_ref, w_ref, qg_ref, kg_ref, cw_ref, dw_ref, iw_ref, dp_ref, de_hbm, forget_ref, ag_ref, rg_ref, wa_hbm,
    wr_hbm, out_ref, de_ref, wa_ref, wr_ref, ls, gk, ga, gb, kv0, kv1, st, halo, normed, proj, k0_ref, k1_ref, ends, q_ref, gates, acc, top, cum, loc,
    mixed, terms, held, send, recv, hs, hr, *sems
):
    seqs, rows, depth = q_ref.shape
    span = k0_ref.shape[1]
    heads = rows // span
    wide = span + HALO
    ck, ca, cb = gk.shape[-1], ga.shape[-1], gb.shape[-1]
    first_w = Torus([(w_ref.at[:, pl.ds(0, ck)], gk, "y")], sems[:6])
    more_w = Torus([(w_ref.at[:, pl.ds(ck, ca)], ga, "y"), (w_ref.at[:, pl.ds(ck + ca, cb)], gb, "z")], sems[6:12])
    keys = Torus([(k0_ref, kv0, "y"), (k1_ref, kv1, "z")], sems[12:18])
    chain = Torus([(ends, st, "y")], sems[18:])
    me = index_of(keys.z, keys.y, keys.c)
    later, earlier = coords_of(lax.rem(me + 1, 128)), coords_of(lax.rem(me + 127, 128))
    loads = [
        pltpu.make_async_copy(a, b, ls.at[i])
        for i, (a, b) in enumerate(((de_hbm, de_ref), (wa_hbm, wa_ref), (wr_hbm, wr_ref)))
    ]
    for load in loads:
        load.start()
    column = lax.axis_index("tp")
    peers = [lax.rem(column + j, 4) for j in range(4)]
    meet(keys.peers() + [{"tp": p} for p in peers[1:]] + [later, earlier])
    first_w.begin()
    edge = keys.copy(x_ref.at[:, pl.ds(span - HALO, HALO)], halo, hs, hr, later)
    edge.start()
    more_w.begin()

    def norm(values):
        full = values.astype(F32)
        scale = lax.rsqrt(jnp.mean(full * full, axis=-1, keepdims=True) + EPS)
        return (full * scale * gain_ref[...]).astype(BF16)

    for b in range(seqs):
        for r in range(0, span, 32):
            normed[b * wide + HALO + r:b * wide + HALO + r + 32] = norm(x_ref[b, r:r + 32])
    first_w.short_lines()
    edge.wait()
    for b in range(seqs):
        normed[b * wide:b * wide + HALO] = norm(halo[b])
    more_w.lines()
    more_w.step(1)
    first_w.short_finish()
    kv_proj = jnp.dot(normed[...], gk[...].reshape(-1, ck), preferred_element_type=F32)
    for b, k_ref in enumerate((k0_ref, k1_ref)):
        kv = kv_proj[b * wide + HALO:(b + 1) * wide]
        k_ref[...] = jnp.concatenate([head_scale(kv[:, :64], kg_ref[...]), kv[:, 64:]], axis=1).T.astype(BF16)
    keys.begin()
    more_w.step(2)

    first = pl.multiple_of(me * span, span)
    line = 16 * span
    for b in range(seqs):
        base = forget_ref[b, :, pl.ds(first, span)][:, :1]

        def prep(c, _):
            at = pl.multiple_of(c * line, line)
            rel = base - forget_ref[b, :, pl.ds(at, line)]
            pos = at + lax.broadcasted_iota(jnp.int32, rel.shape, 1)
            gates[b, :, pl.ds(at, line)] = gate_pieces(jnp.where(pos < first, rel, -1e30))
            return 0

        lax.fori_loop(0, RING, prep, 0)
    more_w.step(3)
    keys.lines()
    more_w.step(4)
    more_w.own_shared()
    for s in range(1, 5):
        more_w.step_shared(s)
    for g, at, n in ((ga, 0, ca), (gb, ca, cb)):
        proj[:, at:at + n] = jnp.dot(normed[...], g[...].reshape(-1, n), preferred_element_type=F32)

    loads[0].wait()
    power = softplus(-dp_ref[...]) * -8.0
    for b in range(seqs):
        own = pl.ds(b * wide + HALO, span)
        before = proj[b * wide:b * wide + HALO, 256:512] * jnp.where(me > 0, 1.0, 0.0)
        ext = jnp.concatenate([before, proj[own, 256:512]], axis=0).astype(BF16).astype(F32)
        conv = jnp.zeros((span, 256), F32)
        for k in range(4):
            conv = conv + ext[HALO - 3 + k:HALO - 3 + k + span] * cw_ref[k:k + 1].astype(F32)
        conv = conv.astype(BF16)
        gd, gi = (
            jnp.concatenate(
                [jnp.dot(conv[:, n * 64:(n + 1) * 64], w[n], preferred_element_type=F32) for n in range(4)], axis=1
            )
            for w in (dw_ref, iw_ref)
        )
        log_decay = power * jax.nn.sigmoid(gd) + de_ref[b]
        add = jnp.sqrt(one_less_exp(2.0 * log_decay)) * jax.nn.sigmoid(gi) * conv.astype(F32)
        mul = jnp.exp(log_decay)
        s = 1
        while s < span:
            mul_b = jnp.concatenate([jnp.ones((s, 256), F32), mul[:-s]], axis=0)
            add_b = jnp.concatenate([jnp.zeros((s, 256), F32), add[:-s]], axis=0)
            add = mul * add_b + add
            mul = mul * mul_b
            s *= 2
        cum[b] = mul
        loc[b] = add
        ends[0, b:b + 1] = mul[span - 1:]
        ends[1, b:b + 1] = add[span - 1:]
    chain.begin()

    ones_own = jnp.ones((16, span), BF16)
    ones = jnp.ones((16, line), BF16)
    row = lax.broadcasted_iota(jnp.int32, (rows, span), 0) % span
    col = lax.broadcasted_iota(jnp.int32, (rows, span), 1)
    lane = lax.broadcasted_iota(jnp.int32, (span, 16), 1)
    for b, k_ref in enumerate((k0_ref, k1_ref)):
        query = proj[pl.ds(b * wide + HALO, span), :256]
        for h in range(heads):
            q = head_scale(query[:, h * 64:(h + 1) * 64], qg_ref[...]).astype(BF16).astype(F32) * 0.125
            picks = jnp.where((lane % 4 == h) & (lane < 12), 1.0, 0.0)
            q_ref[b, h * span:(h + 1) * span] = jnp.concatenate([q, picks], axis=1).astype(BF16)
        near = forget_ref[b, :, pl.ds(first, span)]
        own = k_ref[...]
        rhs = jnp.concatenate([own[:64], gate_pieces(near[:, :1] - near)], axis=0)
        s = jnp.dot(q_ref[b], rhs, preferred_element_type=F32)
        s = jnp.where(row >= col, s, -jnp.inf)
        m = jnp.max(s, axis=1, keepdims=True)
        p = jnp.exp(s - m).astype(BF16)
        acc[b] = lax.dot_general(p, jnp.concatenate([own[64:], ones_own], axis=0), NT, preferred_element_type=F32)
        top[b] = jnp.broadcast_to(m, (rows, 128))

    def attend(b, parts):
        kv = (kv0, kv1)[b]
        spots = [(j, i, c) if b == 0 else (i, j, c) for j, c in parts for i in range(RING)]
        blocks = [kv[z, y, c] for z, y, c in spots]
        near_gates = [gates[b, :, pl.ds(pl.multiple_of(index_of(z, y, c) * span, span), span)] for z, y, c in spots]
        rhs = jnp.concatenate(
            [jnp.concatenate([x[:64] for x in blocks], axis=1), jnp.concatenate(near_gates, axis=1)], axis=0
        )
        s = jnp.dot(q_ref[b], rhs, preferred_element_type=F32)
        old = top[b][:, :1]
        m = jnp.maximum(old, jnp.max(s, axis=1, keepdims=True))
        p = jnp.exp(s - m).astype(BF16)
        vx = jnp.concatenate([jnp.concatenate([x[64:] for x in blocks], axis=1), ones], axis=0)
        acc[b] = acc[b] * jnp.exp(old - m) + lax.dot_general(p, vx, NT, preferred_element_type=F32)
        top[b] = jnp.broadcast_to(m, (rows, 128))

    def work(b, *parts):
        near = [j * (16 if b == 0 else 2) < me for j, _ in parts]
        pl.when(functools.reduce(jnp.logical_or, near))(lambda: attend(b, parts))

    def sides(b, s, core):
        work(b, *[(keys.back(b, d, s), core) for d in (0, 1)])

    mine, its = keys.c, 1 - keys.c
    keys.step(1)
    keys.own_shared()
    work(0, (keys.z, 0), (keys.z, 1))
    work(1, (keys.y, 0), (keys.y, 1))
    chain.lines()

    def turn(s, _):
        sides(0, s, mine)
        sides(1, s, mine)
        keys.step_shared(s)
        sides(0, s, its)
        sides(1, s, its)
        keys.step(s + 1)
        chain.step(s)
        return 0

    lax.fori_loop(1, 3, turn, 0)
    sides(0, 3, mine)
    sides(1, 3, mine)
    keys.step_shared(3)
    sides(0, 3, its)
    keys.step(4)
    chain.step(3)
    keys.step_shared(4)
    work(0, (keys.back(0, 0, 4), 0), (keys.back(0, 0, 4), 1))
    chain.step(4)
    chain.own_shared()
    for s in range(1, 5):
        chain.step_shared(s)

    def merge(j, state):
        part = st.at[j // 16, lax.rem(j // 2, RING), lax.rem(j, 2)]
        return part[0] * state + part[1]

    entering = lax.fori_loop(0, me, merge, jnp.zeros((2, 256), F32))
    width = out_ref.shape[1]
    loads[1].wait()
    loads[2].wait()
    links = []

    def post(i, src, j):
        copy = keys.copy(src, held.at[i], send.at[i], recv.at[i], {"tp": peers[j]})
        copy.start()
        links.append(copy)

    def products(b, straight):
        a = acc[b]
        att = head_scale(a[:, :64] / a[:, 64:65], 1.0)
        att = jnp.concatenate([att[h * span:(h + 1) * span] for h in range(heads)], axis=1)
        mixed[0] = (att * ag_ref[...]).astype(BF16)
        state = loc[b] + cum[b] * entering[b:b + 1]
        gated = state * jax.nn.gelu(proj[pl.ds(b * wide + HALO, span), 512:])
        rec = jnp.concatenate([head_scale(gated[:, n * 64:(n + 1) * 64], 1.0) for n in range(4)], axis=1)
        mixed[1] = (rec * rg_ref[...]).astype(BF16)
        for j in (2, straight, 4 - straight, 0):
            part = pl.ds(pl.multiple_of(peers[j] * width, width), width)
            total = jnp.dot(mixed[0], wa_ref[:, part], preferred_element_type=F32)
            total = total + jnp.dot(mixed[1], wr_ref[:, part], preferred_element_type=F32)
            terms[b, j] = total.astype(BF16)
            if j == 2:
                post(3 * b, terms.at[b, 2], 4 - straight)
            if j == straight:
                post(3 * b + 1, terms.at[b, j], straight)

    def relay(b, straight):
        links[3 * b].wait_recv()
        onward = terms[b, 4 - straight].astype(F32) + held[3 * b].astype(F32)
        terms[b, 4 - straight] = onward.astype(BF16)
        post(3 * b + 2, terms.at[b, 4 - straight], 4 - straight)

    products(0, 3)
    sides(1, 3, its)
    relay(0, 3)
    work(1, (keys.back(1, 0, 4), 0), (keys.back(1, 0, 4), 1))
    products(1, 1)
    relay(1, 1)
    for group in (first_w, more_w, keys, chain):
        group.drain()
    for b in range(seqs):
        for i in (1, 2):
            links[3 * b + i].wait_recv()
        total = terms[b, 0].astype(F32) + held[3 * b + 1].astype(F32) + held[3 * b + 2].astype(F32)
        out_ref[b * span:(b + 1) * span] = total.astype(BF16)
    for link in links:
        link.wait_send()


def layer(x, gain, w, *more):
    span, length, out_cols = x.shape[1], more[7].shape[2], more[-1].shape[1]
    wide, width = 2 * (span + HALO), out_cols // 4
    dma = pltpu.SemaphoreType.DMA

    def grid(dtype, *shape):
        return pltpu.VMEM((8, 8, 2, *shape), dtype)

    return pl.pallas_call(
        kernel,
        out_shape=jax.ShapeDtypeStruct((2 * span, width), BF16),
        in_specs=[ANY if i in (9, 13, 14) else VMEM for i in range(15)],
        out_specs=VMEM,
        scratch_shapes=[
            pltpu.VMEM((2, span, 256), F32),
            pltpu.VMEM(more[-2].shape, BF16),
            pltpu.VMEM(more[-1].shape, BF16),
            dma((3,)),
            grid(BF16, w.shape[0], 128),
            grid(BF16, w.shape[0], 384),
            grid(BF16, w.shape[0], 384),
            grid(BF16, 128, span),
            grid(BF16, 128, span),
            grid(F32, 2, 2, 256),
            pltpu.VMEM((2, HALO, x.shape[2]), BF16),
            pltpu.VMEM((wide, x.shape[2]), BF16),
            pltpu.VMEM((wide, 768), F32),
            pltpu.VMEM((128, span), BF16),
            pltpu.VMEM((128, span), BF16),
            pltpu.VMEM((2, 2, 256), F32),
            pltpu.VMEM((2, 4 * span, 80), BF16),
            pltpu.VMEM((2, 16, length), BF16),
            pltpu.VMEM((2, 4 * span, 80), F32),
            pltpu.VMEM((2, 4 * span, 128), F32),
            pltpu.VMEM((2, span, 256), F32),
            pltpu.VMEM((2, span, 256), F32),
            pltpu.VMEM((2, span, 256), BF16),
            pltpu.VMEM((2, 4, span, width), BF16),
            pltpu.VMEM((6, span, width), BF16),
            dma((6,)),
            dma((6,)),
            dma,
            dma,
            *torus_sems(1),
            *torus_sems(2),
            *torus_sems(2),
            *torus_sems(1),
        ],
        compiler_params=params(0),
    )(x, gain, w, *more)


def body(
    inputs, norm_gain, query_weight, key_weight, value_weight, query_gain, key_gain, forget_cache, rec_in_weight,
    rec_gate_weight, conv_weight, decay_gate_weight, input_gate_weight, decay_param, decay_extra, attn_out_gain,
    rec_out_gain, out_att_weight, out_rec_weight,
):
    joined = jnp.concatenate([key_weight, value_weight, query_weight, rec_in_weight, rec_gate_weight], axis=1)
    mixed = layer(
        inputs, norm_gain[None], joined, query_gain[None], key_gain[None], conv_weight, decay_gate_weight,
        input_gate_weight, decay_param[None], decay_extra, forget_cache, attn_out_gain[None], rec_out_gain[None],
        out_att_weight, out_rec_weight,
    )
    return mixed.reshape(2, inputs.shape[1], -1)


def solution(mesh):
    finer = Mesh(mesh.devices.reshape(8, 8, 2, mesh.shape["tp"]), (*SP, "tp"))
    return jax.shard_map(
        body,
        mesh=finer,
        in_specs=(
            P(None, SP, None), P(), P(SP, "tp"), P(SP, "tp"), P(SP, "tp"), P(), P(), P(None, "tp", None), P(SP, "tp"),
            P(SP, "tp"), P(None, "tp"), P("tp", None, None), P("tp", None, None), P("tp"), P(None, SP, "tp"), P("tp"),
            P("tp"), P("tp", None), P("tp", None),
        ),
        out_specs=P(None, SP, "tp"),
        check_vma=False,
    )
```

```python
import functools

import jax
import jax.numpy as jnp
from jax import lax
from jax.experimental import pallas as pl
from jax.experimental.pallas import tpu as pltpu
from jax.sharding import Mesh
from jax.sharding import PartitionSpec as P

SP = ("sp_0", "sp_1", "sp_2")
NT = (((1,), (1,)), ((), ()))
EPS = 1e-6
HALO = 16
F32, BF16 = jnp.float32, jnp.bfloat16
VMEM = pl.BlockSpec(memory_space=pltpu.VMEM)
ANY = pl.BlockSpec(memory_space=pl.ANY)

MESH = pl.DeviceIdType.MESH
RING = 8


class Torus:
    def __init__(self, streams, sems):
        self.streams = streams
        self.s1, self.r1, self.s2, self.r2, self.ps, self.pr = sems
        self.z, self.y, self.c = (lax.axis_index(n) for n in SP)
        self.sign = 1 - 2 * self.c
        self.other = {"sp_2": 1 - self.c}
        self.ks = range(len(streams))

    def peers(self):
        found = [self.other]
        for name, pos in (("sp_0", self.z), ("sp_1", self.y)):
            found += [{name: lax.rem(pos + i, RING)} for i in range(1, RING)]
        return found

    def places(self, k):
        return (self.y, self.z) if self.streams[k][2] == "y" else (self.z, self.y)

    def axes(self, k):
        return ("sp_1", "sp_0") if self.streams[k][2] == "y" else ("sp_0", "sp_1")

    def one(self, k, i):
        o, first = self.streams[k][1:]
        return o.at[self.z, i, self.c] if first == "y" else o.at[i, self.y, self.c]

    def line(self, k, j, core):
        o, first = self.streams[k][1:]
        return o.at[j, :, core] if first == "y" else o.at[:, j, core]

    def back(self, k, d, s):
        sg = self.sign if d == 0 else -self.sign
        return lax.rem(self.places(k)[1] - sg * s + RING, RING)

    def copy(self, src, dst, send, recv, device):
        return pltpu.make_async_remote_copy(
            src_ref=src, dst_ref=dst, send_sem=send, recv_sem=recv, device_id=device, device_id_type=MESH
        )

    def arrived(self, ref, send, recv):
        self.copy(ref, ref, send, recv, self.other).wait_recv()

    def begin(self):
        for i in (4, 5, 3, 6, 2, 7, 1):
            for k in self.ks:
                pos = self.places(k)[0]
                self.copy(
                    self.streams[k][0], self.one(k, pos), self.s1.at[k, i - 1], self.r1.at[k, i - 1],
                    {self.axes(k)[0]: lax.rem(pos + i, RING)},
                ).start()
        for k in self.ks:
            self.streams[k][1][self.z, self.y, self.c] = self.streams[k][0][...]

    def joined(self, k):
        pos = self.places(k)[0]
        for i in range(1, RING):
            got = self.one(k, lax.rem(pos + RING - i, RING))
            self.arrived(got, self.s1.at[k, i - 1], self.r1.at[k, i - 1])

    def pass_on(self, k, d, s):
        ref = self.line(k, self.back(k, d, s - 1), self.c)
        device = {self.axes(k)[1]: self.back(k, d, -1)}
        self.copy(ref, ref, self.s2.at[k, d, s - 1], self.r2.at[k, d, s - 1], device).start()

    def share(self, k, j, d, s):
        ref = self.line(k, j, self.c)
        self.copy(ref, ref, self.ps.at[k, d, s], self.pr.at[k, d, s], self.other).start()

    def shared(self, k, j, d, s):
        self.arrived(self.line(k, j, 1 - self.c), self.ps.at[k, d, s], self.pr.at[k, d, s])

    def lines(self):
        for k in self.ks:
            self.joined(k)
            for d in (0, 1):
                self.pass_on(k, d, 1)
            self.share(k, self.places(k)[1], 0, 0)

    def step(self, s):
        for k in self.ks:
            for d in (0, 1):
                if not isinstance(s, int) or s + d <= 4:
                    got = self.line(k, self.back(k, d, s), self.c)
                    self.arrived(got, self.s2.at[k, d, s - 1], self.r2.at[k, d, s - 1])
                    if isinstance(s, int):
                        if s + d < 4:
                            self.pass_on(k, d, s + 1)
                    else:
                        pl.when(s + d < 4)(functools.partial(self.pass_on, k, d, s + 1))
                    self.share(k, self.back(k, d, s), d, s)

    def step_shared(self, s):
        for k in self.ks:
            for d in (0, 1):
                if not isinstance(s, int) or s + d <= 4:
                    self.shared(k, self.back(k, d, -s), d, s)

    def own_shared(self):
        for k in self.ks:
            self.shared(k, self.places(k)[1], 0, 0)

    def drain(self):
        for k in self.ks:
            one, line = self.streams[k][0], self.line(k, self.places(k)[1], self.c)
            for i in range(7):
                self.copy(one, one, self.s1.at[k, i], self.r1.at[k, i], self.other).wait_send()
            self.copy(line, line, self.ps.at[k, 0, 0], self.pr.at[k, 0, 0], self.other).wait_send()
            for i in range(7):
                d, s = i // 4, i % 4
                self.copy(line, line, self.s2.at[k, d, s], self.r2.at[k, d, s], self.other).wait_send()
                self.copy(line, line, self.ps.at[k, d, s + 1], self.pr.at[k, d, s + 1], self.other).wait_send()

    def short_lines(self):
        for k in self.ks:
            self.joined(k)
            pos = self.places(k)[1]
            ref = self.line(k, pos, self.c)
            for i in (4, 5, 3, 6, 2, 7, 1):
                d, s = (i - 1) // 4, (i - 1) % 4
                device = {self.axes(k)[1]: lax.rem(pos + i, RING)}
                self.copy(ref, ref, self.s2.at[k, d, s], self.r2.at[k, d, s], device).start()
            self.share(k, pos, 0, 0)

    def short_finish(self):
        for k in self.ks:
            pos = self.places(k)[1]
            for i in (1, 7, 2, 6, 3, 5, 4):
                d, s = (i - 1) // 4, (i - 1) % 4
                j = lax.rem(pos + RING - i, RING)
                self.arrived(self.line(k, j, self.c), self.s2.at[k, d, s], self.r2.at[k, d, s])
                self.share(k, j, d, s + 1)
            self.shared(k, pos, 0, 0)
            for i in range(1, RING):
                self.shared(k, lax.rem(pos + RING - i, RING), (i - 1) // 4, (i - 1) % 4 + 1)


def torus_sems(n):
    dma = pltpu.SemaphoreType.DMA
    return [dma((n, 7)), dma((n, 7)), dma((n, 2, 4)), dma((n, 2, 4)), dma((n, 2, 5)), dma((n, 2, 5))]


def meet(devices):
    barrier = pltpu.get_barrier_semaphore()
    for device in devices:
        pl.semaphore_signal(barrier, inc=1, device_id=device, device_id_type=MESH)
    pl.semaphore_wait(barrier, len(devices))

def params(collective_id=None):
    more = {} if collective_id is None else {"collective_id": collective_id, "has_side_effects": True}
    return pltpu.CompilerParams(vmem_limit_bytes=60 * 1024 * 1024, **more)


def index_of(z, y, c):
    return (z * RING + y) * 2 + c


def coords_of(index):
    return {"sp_0": index // 16, "sp_1": lax.rem(index // 2, RING), "sp_2": lax.rem(index, 2)}


def head_scale(values, gain):
    return values * lax.rsqrt(jnp.mean(values * values, axis=-1, keepdims=True) + EPS) * gain


def softplus(values):
    grown = jnp.exp(-jnp.abs(values))
    series = jnp.zeros_like(grown)
    for n in range(8, 0, -1):
        series = grown * ((1.0 if n % 2 else -1.0) / n + series)
    return jnp.maximum(values, 0.0) + jnp.where(grown < 0.06, series, jnp.log(1.0 + grown))


def one_less_exp(values):
    series = jnp.zeros_like(values)
    for n in range(8, 0, -1):
        series = values / n * (1.0 + series)
    return jnp.where(values > -0.3, -series, 1.0 - jnp.exp(values))


def gate_pieces(rel):
    hi = rel.astype(BF16).astype(F32)
    mid = (rel - hi).astype(BF16).astype(F32)
    return jnp.concatenate([hi, mid, rel - hi - mid, jnp.zeros_like(rel)], axis=0).astype(BF16)


def kernel(
    x_ref, gain_ref, w_ref, qg_ref, kg_ref, cw_ref, dw_ref, iw_ref, dp_ref, de_hbm, forget_ref, ag_ref, rg_ref, wa_hbm,
    wr_hbm, out_ref, de_ref, wa_ref, wr_ref, ls, gk, ga, gb, kv0, kv1, st, halo, normed, proj, k0_ref, k1_ref, ends, q_ref, gates, acc, top, cum, loc,
    mixed, terms, held, send, recv, hs, hr, *sems
):
    seqs, rows, depth = q_ref.shape
    span = k0_ref.shape[1]
    heads = rows // span
    wide = span + HALO
    ck, ca, cb = gk.shape[-1], ga.shape[-1], gb.shape[-1]
    first_w = Torus([(w_ref.at[:, pl.ds(0, ck)], gk, "y")], sems[:6])
    more_w = Torus([(w_ref.at[:, pl.ds(ck, ca)], ga, "y"), (w_ref.at[:, pl.ds(ck + ca, cb)], gb, "z")], sems[6:12])
    keys = Torus([(k0_ref, kv0, "y"), (k1_ref, kv1, "z")], sems[12:18])
    chain = Torus([(ends, st, "y")], sems[18:])
    me = index_of(keys.z, keys.y, keys.c)
    later, earlier = coords_of(lax.rem(me + 1, 128)), coords_of(lax.rem(me + 127, 128))
    loads = [
        pltpu.make_async_copy(a, b, ls.at[i])
        for i, (a, b) in enumerate(((de_hbm, de_ref), (wa_hbm, wa_ref), (wr_hbm, wr_ref)))
    ]
    for load in loads:
        load.start()
    column = lax.axis_index("tp")
    peers = [lax.rem(column + j, 4) for j in range(4)]
    meet(keys.peers() + [{"tp": p} for p in peers[1:]] + [later, earlier])
    first_w.begin()
    edge = keys.copy(x_ref.at[:, pl.ds(span - HALO, HALO)], halo, hs, hr, later)
    edge.start()
    more_w.begin()

    def norm(values):
        full = values.astype(F32)
        scale = lax.rsqrt(jnp.mean(full * full, axis=-1, keepdims=True) + EPS)
        return (full * scale * gain_ref[...]).astype(BF16)

    for b in range(seqs):
        for r in range(0, span, 32):
            normed[b * wide + HALO + r:b * wide + HALO + r + 32] = norm(x_ref[b, r:r + 32])
    first_w.short_lines()
    edge.wait()
    for b in range(seqs):
        normed[b * wide:b * wide + HALO] = norm(halo[b])
    more_w.lines()
    more_w.step(1)
    first_w.short_finish()
    kv_proj = jnp.dot(normed[...], gk[...].reshape(-1, ck), preferred_element_type=F32)
    for b, k_ref in enumerate((k0_ref, k1_ref)):
        kv = kv_proj[b * wide + HALO:(b + 1) * wide]
        k_ref[...] = jnp.concatenate([head_scale(kv[:, :64], kg_ref[...]), kv[:, 64:]], axis=1).T.astype(BF16)
    keys.begin()
    more_w.step(2)

    first = pl.multiple_of(me * span, span)
    line = 16 * span
    for b in range(seqs):
        base = forget_ref[b, :, pl.ds(first, span)][:, :1]

        def prep(c, _):
            at = pl.multiple_of(c * line, line)
            rel = base - forget_ref[b, :, pl.ds(at, line)]
            pos = at + lax.broadcasted_iota(jnp.int32, rel.shape, 1)
            gates[b, :, pl.ds(at, line)] = gate_pieces(jnp.where(pos < first, rel, -1e30))
            return 0

        lax.fori_loop(0, RING, prep, 0)
    more_w.step(3)
    keys.lines()
    more_w.step(4)
    more_w.own_shared()
    for s in range(1, 5):
        more_w.step_shared(s)
    for g, at, n in ((ga, 0, ca), (gb, ca, cb)):
        proj[:, at:at + n] = jnp.dot(normed[...], g[...].reshape(-1, n), preferred_element_type=F32)

    loads[0].wait()
    power = softplus(-dp_ref[...]) * -8.0
    for b in range(seqs):
        own = pl.ds(b * wide + HALO, span)
        before = proj[b * wide:b * wide + HALO, 256:512] * jnp.where(me > 0, 1.0, 0.0)
        ext = jnp.concatenate([before, proj[own, 256:512]], axis=0).astype(BF16).astype(F32)
        conv = jnp.zeros((span, 256), F32)
        for k in range(4):
            conv = conv + ext[HALO - 3 + k:HALO - 3 + k + span] * cw_ref[k:k + 1].astype(F32)
        conv = conv.astype(BF16)
        gd, gi = (
            jnp.concatenate(
                [jnp.dot(conv[:, n * 64:(n + 1) * 64], w[n], preferred_element_type=F32) for n in range(4)], axis=1
            )
            for w in (dw_ref, iw_ref)
        )
        log_decay = power * jax.nn.sigmoid(gd) + de_ref[b]
        add = jnp.sqrt(one_less_exp(2.0 * log_decay)) * jax.nn.sigmoid(gi) * conv.astype(F32)
        mul = jnp.exp(log_decay)
        s = 1
        while s < span:
            mul_b = jnp.concatenate([jnp.ones((s, 256), F32), mul[:-s]], axis=0)
            add_b = jnp.concatenate([jnp.zeros((s, 256), F32), add[:-s]], axis=0)
            add = mul * add_b + add
            mul = mul * mul_b
            s *= 2
        cum[b] = mul
        loc[b] = add
        ends[0, b:b + 1] = mul[span - 1:]
        ends[1, b:b + 1] = add[span - 1:]
    chain.begin()

    ones_own = jnp.ones((16, span), BF16)
    ones = jnp.ones((16, line), BF16)
    row = lax.broadcasted_iota(jnp.int32, (rows, span), 0) % span
    col = lax.broadcasted_iota(jnp.int32, (rows, span), 1)
    lane = lax.broadcasted_iota(jnp.int32, (span, 16), 1)
    for b, k_ref in enumerate((k0_ref, k1_ref)):
        query = proj[pl.ds(b * wide + HALO, span), :256]
        for h in range(heads):
            q = head_scale(query[:, h * 64:(h + 1) * 64], qg_ref[...]).astype(BF16).astype(F32) * 0.125
            picks = jnp.where((lane % 4 == h) & (lane < 12), 1.0, 0.0)
            q_ref[b, h * span:(h + 1) * span] = jnp.concatenate([q, picks], axis=1).astype(BF16)
        near = forget_ref[b, :, pl.ds(first, span)]
        own = k_ref[...]
        rhs = jnp.concatenate([own[:64], gate_pieces(near[:, :1] - near)], axis=0)
        s = jnp.dot(q_ref[b], rhs, preferred_element_type=F32)
        s = jnp.where(row >= col, s, -jnp.inf)
        m = jnp.max(s, axis=1, keepdims=True)
        p = jnp.exp(s - m).astype(BF16)
        acc[b] = lax.dot_general(p, jnp.concatenate([own[64:], ones_own], axis=0), NT, preferred_element_type=F32)
        top[b] = jnp.broadcast_to(m, (rows, 128))

    def attend(b, parts):
        kv = (kv0, kv1)[b]
        spots = [(j, i, c) if b == 0 else (i, j, c) for j, c in parts for i in range(RING)]
        blocks = [kv[z, y, c] for z, y, c in spots]
        near_gates = [gates[b, :, pl.ds(pl.multiple_of(index_of(z, y, c) * span, span), span)] for z, y, c in spots]
        rhs = jnp.concatenate(
            [jnp.concatenate([x[:64] for x in blocks], axis=1), jnp.concatenate(near_gates, axis=1)], axis=0
        )
        vx = jnp.concatenate([jnp.concatenate([x[64:] for x in blocks], axis=1), ones], axis=0)
        half = rows // 2
        starts = (0, half)
        scores = [jnp.dot(q_ref[b, at:at + half], rhs, preferred_element_type=F32) for at in starts]
        for at, s in zip(starts, scores):
            old = top[b, at:at + half][:, :1]
            m = jnp.maximum(old, jnp.max(s, axis=1, keepdims=True))
            p = jnp.exp(s - m).astype(BF16)
            fresh = lax.dot_general(p, vx, NT, preferred_element_type=F32)
            acc[b, at:at + half] = acc[b, at:at + half] * jnp.exp(old - m) + fresh
            top[b, at:at + half] = jnp.broadcast_to(m, (half, 128))

    def work(b, *parts):
        near = [j * (16 if b == 0 else 2) < me for j, _ in parts]
        pl.when(functools.reduce(jnp.logical_or, near))(lambda: attend(b, parts))

    def sides(b, s, core):
        work(b, *[(keys.back(b, d, s), core) for d in (0, 1)])

    mine, its = keys.c, 1 - keys.c
    keys.step(1)
    keys.own_shared()
    work(0, (keys.z, 0), (keys.z, 1))
    work(1, (keys.y, 0), (keys.y, 1))
    chain.lines()

    def turn(s, _):
        sides(0, s, mine)
        sides(1, s, mine)
        keys.step_shared(s)
        sides(0, s, its)
        sides(1, s, its)
        keys.step(s + 1)
        chain.step(s)
        return 0

    lax.fori_loop(1, 3, turn, 0)
    sides(0, 3, mine)
    sides(1, 3, mine)
    keys.step_shared(3)
    sides(0, 3, its)
    keys.step(4)
    chain.step(3)
    keys.step_shared(4)
    work(0, (keys.back(0, 0, 4), 0), (keys.back(0, 0, 4), 1))
    chain.step(4)
    chain.own_shared()
    for s in range(1, 5):
        chain.step_shared(s)

    places = lax.broadcasted_iota(jnp.int32, (RING, 2, 256), 0) * 16
    decay, state = jnp.ones((RING, 2, 256), F32), jnp.zeros((RING, 2, 256), F32)
    for i in range(16):
        before = places + i < me
        shrink = jnp.where(before, st[:, i // 2, i % 2, 0], 1.0)
        state = shrink * state + jnp.where(before, st[:, i // 2, i % 2, 1], 0.0)
        decay = shrink * decay
    entering = jnp.zeros((2, 256), F32)
    for z in range(RING):
        entering = decay[z] * entering + state[z]
    width = out_ref.shape[1]
    loads[1].wait()
    loads[2].wait()
    links = []

    def post(i, src, j):
        copy = keys.copy(src, held.at[i], send.at[i], recv.at[i], {"tp": peers[j]})
        copy.start()
        links.append(copy)

    def products(b, straight):
        a = acc[b]
        att = head_scale(a[:, :64] / a[:, 64:65], 1.0)
        att = jnp.concatenate([att[h * span:(h + 1) * span] for h in range(heads)], axis=1)
        mixed[0] = (att * ag_ref[...]).astype(BF16)
        state = loc[b] + cum[b] * entering[b:b + 1]
        gated = state * jax.nn.gelu(proj[pl.ds(b * wide + HALO, span), 512:])
        rec = jnp.concatenate([head_scale(gated[:, n * 64:(n + 1) * 64], 1.0) for n in range(4)], axis=1)
        mixed[1] = (rec * rg_ref[...]).astype(BF16)
        for j in (2, straight, 4 - straight, 0):
            part = pl.ds(pl.multiple_of(peers[j] * width, width), width)
            total = jnp.dot(mixed[0], wa_ref[:, part], preferred_element_type=F32)
            total = total + jnp.dot(mixed[1], wr_ref[:, part], preferred_element_type=F32)
            terms[b, j] = total.astype(BF16)
            if j == 2:
                post(3 * b, terms.at[b, 2], 4 - straight)
            if j == straight:
                post(3 * b + 1, terms.at[b, j], straight)

    def relay(b, straight):
        links[3 * b].wait_recv()
        onward = terms[b, 4 - straight].astype(F32) + held[3 * b].astype(F32)
        terms[b, 4 - straight] = onward.astype(BF16)
        post(3 * b + 2, terms.at[b, 4 - straight], 4 - straight)

    products(0, 3)
    sides(1, 3, its)
    work(1, (keys.back(1, 0, 4), 0), (keys.back(1, 0, 4), 1))
    relay(0, 3)
    products(1, 1)
    relay(1, 1)
    for group in (first_w, more_w, keys, chain):
        group.drain()
    for b in range(seqs):
        for i in (1, 2):
            links[3 * b + i].wait_recv()
        total = terms[b, 0].astype(F32) + held[3 * b + 1].astype(F32) + held[3 * b + 2].astype(F32)
        out_ref[b * span:(b + 1) * span] = total.astype(BF16)
    for link in links:
        link.wait_send()


def layer(x, gain, w, *more):
    span, length, out_cols = x.shape[1], more[7].shape[2], more[-1].shape[1]
    wide, width = 2 * (span + HALO), out_cols // 4
    dma = pltpu.SemaphoreType.DMA

    def grid(dtype, *shape):
        return pltpu.VMEM((8, 8, 2, *shape), dtype)

    return pl.pallas_call(
        kernel,
        out_shape=jax.ShapeDtypeStruct((2 * span, width), BF16),
        in_specs=[ANY if i in (9, 13, 14) else VMEM for i in range(15)],
        out_specs=VMEM,
        scratch_shapes=[
            pltpu.VMEM((2, span, 256), F32),
            pltpu.VMEM(more[-2].shape, BF16),
            pltpu.VMEM(more[-1].shape, BF16),
            dma((3,)),
            grid(BF16, w.shape[0], 128),
            grid(BF16, w.shape[0], 384),
            grid(BF16, w.shape[0], 384),
            grid(BF16, 128, span),
            grid(BF16, 128, span),
            grid(F32, 2, 2, 256),
            pltpu.VMEM((2, HALO, x.shape[2]), BF16),
            pltpu.VMEM((wide, x.shape[2]), BF16),
            pltpu.VMEM((wide, 768), F32),
            pltpu.VMEM((128, span), BF16),
            pltpu.VMEM((128, span), BF16),
            pltpu.VMEM((2, 2, 256), F32),
            pltpu.VMEM((2, 4 * span, 80), BF16),
            pltpu.VMEM((2, 16, length), BF16),
            pltpu.VMEM((2, 4 * span, 80), F32),
            pltpu.VMEM((2, 4 * span, 128), F32),
            pltpu.VMEM((2, span, 256), F32),
            pltpu.VMEM((2, span, 256), F32),
            pltpu.VMEM((2, span, 256), BF16),
            pltpu.VMEM((2, 4, span, width), BF16),
            pltpu.VMEM((6, span, width), BF16),
            dma((6,)),
            dma((6,)),
            dma,
            dma,
            *torus_sems(1),
            *torus_sems(2),
            *torus_sems(2),
            *torus_sems(1),
        ],
        compiler_params=params(0),
    )(x, gain, w, *more)


def body(
    inputs, norm_gain, query_weight, key_weight, value_weight, query_gain, key_gain, forget_cache, rec_in_weight,
    rec_gate_weight, conv_weight, decay_gate_weight, input_gate_weight, decay_param, decay_extra, attn_out_gain,
    rec_out_gain, out_att_weight, out_rec_weight,
):
    joined = jnp.concatenate([key_weight, value_weight, query_weight, rec_in_weight, rec_gate_weight], axis=1)
    mixed = layer(
        inputs, norm_gain[None], joined, query_gain[None], key_gain[None], conv_weight, decay_gate_weight,
        input_gate_weight, decay_param[None], decay_extra, forget_cache, attn_out_gain[None], rec_out_gain[None],
        out_att_weight, out_rec_weight,
    )
    return mixed.reshape(2, inputs.shape[1], -1)


def solution(mesh):
    finer = Mesh(mesh.devices.reshape(8, 8, 2, mesh.shape["tp"]), (*SP, "tp"))
    return jax.shard_map(
        body,
        mesh=finer,
        in_specs=(
            P(None, SP, None), P(), P(SP, "tp"), P(SP, "tp"), P(SP, "tp"), P(), P(), P(None, "tp", None), P(SP, "tp"),
            P(SP, "tp"), P(None, "tp"), P("tp", None, None), P("tp", None, None), P("tp"), P(None, SP, "tp"), P("tp"),
            P("tp"), P("tp", None), P("tp", None),
        ),
        out_specs=P(None, SP, "tp"),
        check_vma=False,
    )
```

```python
import functools

import jax
import jax.numpy as jnp
from jax import lax
from jax.experimental import pallas as pl
from jax.experimental.pallas import tpu as pltpu
from jax.sharding import Mesh
from jax.sharding import PartitionSpec as P

SP = ("sp_0", "sp_1", "sp_2")
NT = (((1,), (1,)), ((), ()))
EPS = 1e-6
HALO = 16
F32, BF16 = jnp.float32, jnp.bfloat16
VMEM = pl.BlockSpec(memory_space=pltpu.VMEM)
ANY = pl.BlockSpec(memory_space=pl.ANY)

MESH = pl.DeviceIdType.MESH
RING = 8


class Torus:
    def __init__(self, streams, sems):
        self.streams = streams
        self.s1, self.r1, self.s2, self.r2, self.ps, self.pr = sems
        self.z, self.y, self.c = (lax.axis_index(n) for n in SP)
        self.sign = 1 - 2 * self.c
        self.other = {"sp_2": 1 - self.c}
        self.ks = range(len(streams))

    def peers(self):
        found = [self.other]
        for name, pos in (("sp_0", self.z), ("sp_1", self.y)):
            found += [{name: lax.rem(pos + i, RING)} for i in range(1, RING)]
        return found

    def places(self, k):
        return (self.y, self.z) if self.streams[k][2] == "y" else (self.z, self.y)

    def axes(self, k):
        return ("sp_1", "sp_0") if self.streams[k][2] == "y" else ("sp_0", "sp_1")

    def one(self, k, i):
        o, first = self.streams[k][1:]
        return o.at[self.z, i, self.c] if first == "y" else o.at[i, self.y, self.c]

    def line(self, k, j, core):
        o, first = self.streams[k][1:]
        return o.at[j, :, core] if first == "y" else o.at[:, j, core]

    def back(self, k, d, s):
        sg = self.sign if d == 0 else -self.sign
        return lax.rem(self.places(k)[1] - sg * s + RING, RING)

    def copy(self, src, dst, send, recv, device):
        return pltpu.make_async_remote_copy(
            src_ref=src, dst_ref=dst, send_sem=send, recv_sem=recv, device_id=device, device_id_type=MESH
        )

    def arrived(self, ref, send, recv):
        self.copy(ref, ref, send, recv, self.other).wait_recv()

    def begin(self):
        for i in (4, 5, 3, 6, 2, 7, 1):
            for k in self.ks:
                pos = self.places(k)[0]
                self.copy(
                    self.streams[k][0], self.one(k, pos), self.s1.at[k, i - 1], self.r1.at[k, i - 1],
                    {self.axes(k)[0]: lax.rem(pos + i, RING)},
                ).start()
        for k in self.ks:
            self.streams[k][1][self.z, self.y, self.c] = self.streams[k][0][...]

    def joined(self, k):
        pos = self.places(k)[0]
        for i in range(1, RING):
            got = self.one(k, lax.rem(pos + RING - i, RING))
            self.arrived(got, self.s1.at[k, i - 1], self.r1.at[k, i - 1])

    def pass_on(self, k, d, s):
        ref = self.line(k, self.back(k, d, s - 1), self.c)
        device = {self.axes(k)[1]: self.back(k, d, -1)}
        self.copy(ref, ref, self.s2.at[k, d, s - 1], self.r2.at[k, d, s - 1], device).start()

    def share(self, k, j, d, s):
        ref = self.line(k, j, self.c)
        self.copy(ref, ref, self.ps.at[k, d, s], self.pr.at[k, d, s], self.other).start()

    def shared(self, k, j, d, s):
        self.arrived(self.line(k, j, 1 - self.c), self.ps.at[k, d, s], self.pr.at[k, d, s])

    def lines(self):
        for k in self.ks:
            self.joined(k)
            for d in (0, 1):
                self.pass_on(k, d, 1)
            self.share(k, self.places(k)[1], 0, 0)

    def step(self, s):
        for k in self.ks:
            for d in (0, 1):
                if not isinstance(s, int) or s + d <= 4:
                    got = self.line(k, self.back(k, d, s), self.c)
                    self.arrived(got, self.s2.at[k, d, s - 1], self.r2.at[k, d, s - 1])
                    if isinstance(s, int):
                        if s + d < 4:
                            self.pass_on(k, d, s + 1)
                    else:
                        pl.when(s + d < 4)(functools.partial(self.pass_on, k, d, s + 1))
                    self.share(k, self.back(k, d, s), d, s)

    def step_shared(self, s):
        for k in self.ks:
            for d in (0, 1):
                if not isinstance(s, int) or s + d <= 4:
                    self.shared(k, self.back(k, d, -s), d, s)

    def own_shared(self):
        for k in self.ks:
            self.shared(k, self.places(k)[1], 0, 0)

    def drain(self):
        for k in self.ks:
            one, line = self.streams[k][0], self.line(k, self.places(k)[1], self.c)
            for i in range(7):
                self.copy(one, one, self.s1.at[k, i], self.r1.at[k, i], self.other).wait_send()
            self.copy(line, line, self.ps.at[k, 0, 0], self.pr.at[k, 0, 0], self.other).wait_send()
            for i in range(7):
                d, s = i // 4, i % 4
                self.copy(line, line, self.s2.at[k, d, s], self.r2.at[k, d, s], self.other).wait_send()
                self.copy(line, line, self.ps.at[k, d, s + 1], self.pr.at[k, d, s + 1], self.other).wait_send()

    def short_lines(self):
        for k in self.ks:
            self.joined(k)
            pos = self.places(k)[1]
            ref = self.line(k, pos, self.c)
            for i in (4, 5, 3, 6, 2, 7, 1):
                d, s = (i - 1) // 4, (i - 1) % 4
                device = {self.axes(k)[1]: lax.rem(pos + i, RING)}
                self.copy(ref, ref, self.s2.at[k, d, s], self.r2.at[k, d, s], device).start()
            self.share(k, pos, 0, 0)

    def short_finish(self):
        for k in self.ks:
            pos = self.places(k)[1]
            for i in (1, 7, 2, 6, 3, 5, 4):
                d, s = (i - 1) // 4, (i - 1) % 4
                j = lax.rem(pos + RING - i, RING)
                self.arrived(self.line(k, j, self.c), self.s2.at[k, d, s], self.r2.at[k, d, s])
                self.share(k, j, d, s + 1)
            self.shared(k, pos, 0, 0)
            for i in range(1, RING):
                self.shared(k, lax.rem(pos + RING - i, RING), (i - 1) // 4, (i - 1) % 4 + 1)


def torus_sems(n):
    dma = pltpu.SemaphoreType.DMA
    return [dma((n, 7)), dma((n, 7)), dma((n, 2, 4)), dma((n, 2, 4)), dma((n, 2, 5)), dma((n, 2, 5))]


def meet(devices):
    barrier = pltpu.get_barrier_semaphore()
    for device in devices:
        pl.semaphore_signal(barrier, inc=1, device_id=device, device_id_type=MESH)
    pl.semaphore_wait(barrier, len(devices))

def params(collective_id=None):
    more = {} if collective_id is None else {"collective_id": collective_id, "has_side_effects": True}
    return pltpu.CompilerParams(vmem_limit_bytes=60 * 1024 * 1024, **more)


def index_of(z, y, c):
    return (z * RING + y) * 2 + c


def coords_of(index):
    return {"sp_0": index // 16, "sp_1": lax.rem(index // 2, RING), "sp_2": lax.rem(index, 2)}


def head_scale(values, gain):
    return values * lax.rsqrt(jnp.mean(values * values, axis=-1, keepdims=True) + EPS) * gain


def softplus(values):
    grown = jnp.exp(-jnp.abs(values))
    series = jnp.zeros_like(grown)
    for n in range(8, 0, -1):
        series = grown * ((1.0 if n % 2 else -1.0) / n + series)
    return jnp.maximum(values, 0.0) + jnp.where(grown < 0.06, series, jnp.log(1.0 + grown))


def one_less_exp(values):
    series = jnp.zeros_like(values)
    for n in range(8, 0, -1):
        series = values / n * (1.0 + series)
    return jnp.where(values > -0.3, -series, 1.0 - jnp.exp(values))


def gate_pieces(rel):
    hi = rel.astype(BF16).astype(F32)
    mid = (rel - hi).astype(BF16).astype(F32)
    return jnp.concatenate([hi, mid, rel - hi - mid, jnp.zeros_like(rel)], axis=0).astype(BF16)


def kernel(
    x_ref, gain_ref, w_ref, qg_ref, kg_ref, cw_ref, dw_ref, iw_ref, dp_ref, de_hbm, forget_ref, ag_ref, rg_ref, wa_hbm,
    wr_hbm, out_ref, de_ref, wa_ref, wr_ref, ls, gk, ga, gb, kv0, kv1, st, halo, normed, proj, k0_ref, k1_ref, ends, q_ref, gates, acc, top, cum, loc,
    mixed, terms, held, send, recv, hs, hr, *sems
):
    seqs, rows, depth = q_ref.shape
    span = k0_ref.shape[1]
    heads = rows // span
    wide = span + HALO
    ck, ca, cb = gk.shape[-1], ga.shape[-1], gb.shape[-1]
    first_w = Torus([(w_ref.at[:, pl.ds(0, ck)], gk, "y")], sems[:6])
    more_w = Torus([(w_ref.at[:, pl.ds(ck, ca)], ga, "y"), (w_ref.at[:, pl.ds(ck + ca, cb)], gb, "z")], sems[6:12])
    keys = Torus([(k0_ref, kv0, "y"), (k1_ref, kv1, "z")], sems[12:18])
    chain = Torus([(ends, st, "y")], sems[18:])
    me = index_of(keys.z, keys.y, keys.c)
    later, earlier = coords_of(lax.rem(me + 1, 128)), coords_of(lax.rem(me + 127, 128))
    loads = [
        pltpu.make_async_copy(a, b, ls.at[i])
        for i, (a, b) in enumerate(((de_hbm, de_ref), (wa_hbm, wa_ref), (wr_hbm, wr_ref)))
    ]
    for load in loads:
        load.start()
    column = lax.axis_index("tp")
    peers = [lax.rem(column + j, 4) for j in range(4)]
    meet(keys.peers() + [{"tp": p} for p in peers[1:]] + [later, earlier])
    first_w.begin()
    edge = keys.copy(x_ref.at[:, pl.ds(span - HALO, HALO)], halo, hs, hr, later)
    edge.start()
    more_w.begin()

    def norm(values):
        full = values.astype(F32)
        scale = lax.rsqrt(jnp.mean(full * full, axis=-1, keepdims=True) + EPS)
        return (full * scale * gain_ref[...]).astype(BF16)

    for b in range(seqs):
        for r in range(0, span, 32):
            normed[b * wide + HALO + r:b * wide + HALO + r + 32] = norm(x_ref[b, r:r + 32])
    first_w.short_lines()
    edge.wait()
    for b in range(seqs):
        normed[b * wide:b * wide + HALO] = norm(halo[b])
    more_w.lines()
    more_w.step(1)
    first_w.short_finish()
    kv_proj = jnp.dot(normed[...], gk[...].reshape(-1, ck), preferred_element_type=F32)
    for b, k_ref in enumerate((k0_ref, k1_ref)):
        kv = kv_proj[b * wide + HALO:(b + 1) * wide]
        k_ref[...] = jnp.concatenate([head_scale(kv[:, :64], kg_ref[...]), kv[:, 64:]], axis=1).T.astype(BF16)
    keys.begin()
    more_w.step(2)

    first = pl.multiple_of(me * span, span)
    line = 16 * span
    for b in range(seqs):
        base = forget_ref[b, :, pl.ds(first, span)][:, :1]

        def prep(c, _):
            at = pl.multiple_of(c * line, line)
            rel = base - forget_ref[b, :, pl.ds(at, line)]
            pos = at + lax.broadcasted_iota(jnp.int32, rel.shape, 1)
            gates[b, :, pl.ds(at, line)] = gate_pieces(jnp.where(pos < first, rel, -1e30))
            return 0

        lax.fori_loop(0, RING, prep, 0)
    more_w.step(3)
    keys.lines()
    more_w.step(4)
    more_w.own_shared()
    for s in range(1, 5):
        more_w.step_shared(s)
    for g, at, n in ((ga, 0, ca), (gb, ca, cb)):
        proj[:, at:at + n] = jnp.dot(normed[...], g[...].reshape(-1, n), preferred_element_type=F32)

    loads[0].wait()
    power = softplus(-dp_ref[...]) * -8.0
    for b in range(seqs):
        own = pl.ds(b * wide + HALO, span)
        before = proj[b * wide:b * wide + HALO, 256:512] * jnp.where(me > 0, 1.0, 0.0)
        ext = jnp.concatenate([before, proj[own, 256:512]], axis=0).astype(BF16).astype(F32)
        conv = jnp.zeros((span, 256), F32)
        for k in range(4):
            conv = conv + ext[HALO - 3 + k:HALO - 3 + k + span] * cw_ref[k:k + 1].astype(F32)
        conv = conv.astype(BF16)
        gd, gi = (
            jnp.concatenate(
                [jnp.dot(conv[:, n * 64:(n + 1) * 64], w[n], preferred_element_type=F32) for n in range(4)], axis=1
            )
            for w in (dw_ref, iw_ref)
        )
        log_decay = power * jax.nn.sigmoid(gd) + de_ref[b]
        add = jnp.sqrt(one_less_exp(2.0 * log_decay)) * jax.nn.sigmoid(gi) * conv.astype(F32)
        mul = jnp.exp(log_decay)
        s = 1
        while s < span:
            mul_b = jnp.concatenate([jnp.ones((s, 256), F32), mul[:-s]], axis=0)
            add_b = jnp.concatenate([jnp.zeros((s, 256), F32), add[:-s]], axis=0)
            add = mul * add_b + add
            mul = mul * mul_b
            s *= 2
        cum[b] = mul
        loc[b] = add
        ends[0, b:b + 1] = mul[span - 1:]
        ends[1, b:b + 1] = add[span - 1:]
    chain.begin()
    keys.step(1)

    ones_own = jnp.ones((16, span), BF16)
    ones = jnp.ones((16, line), BF16)
    row = lax.broadcasted_iota(jnp.int32, (rows, span), 0) % span
    col = lax.broadcasted_iota(jnp.int32, (rows, span), 1)
    lane = lax.broadcasted_iota(jnp.int32, (span, 16), 1)
    for b, k_ref in enumerate((k0_ref, k1_ref)):
        query = proj[pl.ds(b * wide + HALO, span), :256]
        for h in range(heads):
            q = head_scale(query[:, h * 64:(h + 1) * 64], qg_ref[...]).astype(BF16).astype(F32) * 0.125
            picks = jnp.where((lane % 4 == h) & (lane < 12), 1.0, 0.0)
            q_ref[b, h * span:(h + 1) * span] = jnp.concatenate([q, picks], axis=1).astype(BF16)
        near = forget_ref[b, :, pl.ds(first, span)]
        own = k_ref[...]
        rhs = jnp.concatenate([own[:64], gate_pieces(near[:, :1] - near)], axis=0)
        s = jnp.dot(q_ref[b], rhs, preferred_element_type=F32)
        s = jnp.where(row >= col, s, -jnp.inf)
        m = jnp.max(s, axis=1, keepdims=True)
        p = jnp.exp(s - m).astype(BF16)
        acc[b] = lax.dot_general(p, jnp.concatenate([own[64:], ones_own], axis=0), NT, preferred_element_type=F32)
        top[b] = jnp.broadcast_to(m, (rows, 128))

    def attend(b, parts):
        kv = (kv0, kv1)[b]
        spots = [(j, i, c) if b == 0 else (i, j, c) for j, c in parts for i in range(RING)]
        blocks = [kv[z, y, c] for z, y, c in spots]
        near_gates = [gates[b, :, pl.ds(pl.multiple_of(index_of(z, y, c) * span, span), span)] for z, y, c in spots]
        rhs = jnp.concatenate(
            [jnp.concatenate([x[:64] for x in blocks], axis=1), jnp.concatenate(near_gates, axis=1)], axis=0
        )
        vx = jnp.concatenate([jnp.concatenate([x[64:] for x in blocks], axis=1), ones], axis=0)
        half = rows // 2
        starts = (0, half)
        scores = [jnp.dot(q_ref[b, at:at + half], rhs, preferred_element_type=F32) for at in starts]
        for at, s in zip(starts, scores):
            old = top[b, at:at + half][:, :1]
            m = jnp.maximum(old, jnp.max(s, axis=1, keepdims=True))
            p = jnp.exp(s - m).astype(BF16)
            fresh = lax.dot_general(p, vx, NT, preferred_element_type=F32)
            acc[b, at:at + half] = acc[b, at:at + half] * jnp.exp(old - m) + fresh
            top[b, at:at + half] = jnp.broadcast_to(m, (half, 128))

    def work(b, *parts):
        near = [j * (16 if b == 0 else 2) < me for j, _ in parts]
        pl.when(functools.reduce(jnp.logical_or, near))(lambda: attend(b, parts))

    def sides(b, s, core):
        work(b, *[(keys.back(b, d, s), core) for d in (0, 1)])

    mine, its = keys.c, 1 - keys.c
    keys.own_shared()
    work(0, (keys.z, 0), (keys.z, 1))
    work(1, (keys.y, 0), (keys.y, 1))
    chain.lines()

    def turn(s, _):
        sides(0, s, mine)
        sides(1, s, mine)
        keys.step_shared(s)
        sides(0, s, its)
        sides(1, s, its)
        keys.step(s + 1)
        chain.step(s)
        return 0

    lax.fori_loop(1, 3, turn, 0)
    sides(0, 3, mine)
    sides(1, 3, mine)
    keys.step_shared(3)
    sides(0, 3, its)
    keys.step(4)
    chain.step(3)
    keys.step_shared(4)
    work(0, (keys.back(0, 0, 4), 0), (keys.back(0, 0, 4), 1))
    chain.step(4)
    chain.own_shared()
    for s in range(1, 5):
        chain.step_shared(s)

    places = lax.broadcasted_iota(jnp.int32, (RING, 2, 256), 0) * 16
    decay, state = jnp.ones((RING, 2, 256), F32), jnp.zeros((RING, 2, 256), F32)
    for i in range(16):
        before = places + i < me
        shrink = jnp.where(before, st[:, i // 2, i % 2, 0], 1.0)
        state = shrink * state + jnp.where(before, st[:, i // 2, i % 2, 1], 0.0)
        decay = shrink * decay
    entering = jnp.zeros((2, 256), F32)
    for z in range(RING):
        entering = decay[z] * entering + state[z]
    width = out_ref.shape[1]
    loads[1].wait()
    loads[2].wait()
    links = []

    def post(i, src, j):
        copy = keys.copy(src, held.at[i], send.at[i], recv.at[i], {"tp": peers[j]})
        copy.start()
        links.append(copy)

    def products(b, straight):
        a = acc[b]
        att = head_scale(a[:, :64] / a[:, 64:65], 1.0)
        att = jnp.concatenate([att[h * span:(h + 1) * span] for h in range(heads)], axis=1)
        mixed[0] = (att * ag_ref[...]).astype(BF16)
        state = loc[b] + cum[b] * entering[b:b + 1]
        gated = state * jax.nn.gelu(proj[pl.ds(b * wide + HALO, span), 512:])
        rec = jnp.concatenate([head_scale(gated[:, n * 64:(n + 1) * 64], 1.0) for n in range(4)], axis=1)
        mixed[1] = (rec * rg_ref[...]).astype(BF16)
        for j in (2, straight, 4 - straight, 0):
            part = pl.ds(pl.multiple_of(peers[j] * width, width), width)
            total = jnp.dot(mixed[0], wa_ref[:, part], preferred_element_type=F32)
            total = total + jnp.dot(mixed[1], wr_ref[:, part], preferred_element_type=F32)
            terms[b, j] = total.astype(BF16)
            if j == 2:
                post(3 * b, terms.at[b, 2], 4 - straight)
            if j == straight:
                post(3 * b + 1, terms.at[b, j], straight)

    def relay(b, straight):
        links[3 * b].wait_recv()
        onward = terms[b, 4 - straight].astype(F32) + held[3 * b].astype(F32)
        terms[b, 4 - straight] = onward.astype(BF16)
        post(3 * b + 2, terms.at[b, 4 - straight], 4 - straight)

    products(0, 3)
    sides(1, 3, its)
    work(1, (keys.back(1, 0, 4), 0), (keys.back(1, 0, 4), 1))
    relay(0, 3)
    products(1, 1)
    relay(1, 1)
    for group in (first_w, more_w, keys, chain):
        group.drain()
    for b in range(seqs):
        for i in (1, 2):
            links[3 * b + i].wait_recv()
        total = terms[b, 0].astype(F32) + held[3 * b + 1].astype(F32) + held[3 * b + 2].astype(F32)
        out_ref[b * span:(b + 1) * span] = total.astype(BF16)
    for link in links:
        link.wait_send()


def layer(x, gain, w, *more):
    span, length, out_cols = x.shape[1], more[7].shape[2], more[-1].shape[1]
    wide, width = 2 * (span + HALO), out_cols // 4
    dma = pltpu.SemaphoreType.DMA

    def grid(dtype, *shape):
        return pltpu.VMEM((8, 8, 2, *shape), dtype)

    return pl.pallas_call(
        kernel,
        out_shape=jax.ShapeDtypeStruct((2 * span, width), BF16),
        in_specs=[ANY if i in (9, 13, 14) else VMEM for i in range(15)],
        out_specs=VMEM,
        scratch_shapes=[
            pltpu.VMEM((2, span, 256), F32),
            pltpu.VMEM(more[-2].shape, BF16),
            pltpu.VMEM(more[-1].shape, BF16),
            dma((3,)),
            grid(BF16, w.shape[0], 128),
            grid(BF16, w.shape[0], 384),
            grid(BF16, w.shape[0], 384),
            grid(BF16, 128, span),
            grid(BF16, 128, span),
            grid(F32, 2, 2, 256),
            pltpu.VMEM((2, HALO, x.shape[2]), BF16),
            pltpu.VMEM((wide, x.shape[2]), BF16),
            pltpu.VMEM((wide, 768), F32),
            pltpu.VMEM((128, span), BF16),
            pltpu.VMEM((128, span), BF16),
            pltpu.VMEM((2, 2, 256), F32),
            pltpu.VMEM((2, 4 * span, 80), BF16),
            pltpu.VMEM((2, 16, length), BF16),
            pltpu.VMEM((2, 4 * span, 80), F32),
            pltpu.VMEM((2, 4 * span, 128), F32),
            pltpu.VMEM((2, span, 256), F32),
            pltpu.VMEM((2, span, 256), F32),
            pltpu.VMEM((2, span, 256), BF16),
            pltpu.VMEM((2, 4, span, width), BF16),
            pltpu.VMEM((6, span, width), BF16),
            dma((6,)),
            dma((6,)),
            dma,
            dma,
            *torus_sems(1),
            *torus_sems(2),
            *torus_sems(2),
            *torus_sems(1),
        ],
        compiler_params=params(0),
    )(x, gain, w, *more)


def body(
    inputs, norm_gain, query_weight, key_weight, value_weight, query_gain, key_gain, forget_cache, rec_in_weight,
    rec_gate_weight, conv_weight, decay_gate_weight, input_gate_weight, decay_param, decay_extra, attn_out_gain,
    rec_out_gain, out_att_weight, out_rec_weight,
):
    joined = jnp.concatenate([key_weight, value_weight, query_weight, rec_in_weight, rec_gate_weight], axis=1)
    mixed = layer(
        inputs, norm_gain[None], joined, query_gain[None], key_gain[None], conv_weight, decay_gate_weight,
        input_gate_weight, decay_param[None], decay_extra, forget_cache, attn_out_gain[None], rec_out_gain[None],
        out_att_weight, out_rec_weight,
    )
    return mixed.reshape(2, inputs.shape[1], -1)


def solution(mesh):
    finer = Mesh(mesh.devices.reshape(8, 8, 2, mesh.shape["tp"]), (*SP, "tp"))
    return jax.shard_map(
        body,
        mesh=finer,
        in_specs=(
            P(None, SP, None), P(), P(SP, "tp"), P(SP, "tp"), P(SP, "tp"), P(), P(), P(None, "tp", None), P(SP, "tp"),
            P(SP, "tp"), P(None, "tp"), P("tp", None, None), P("tp", None, None), P("tp"), P(None, SP, "tp"), P("tp"),
            P("tp"), P("tp", None), P("tp", None),
        ),
        out_specs=P(None, SP, "tp"),
        check_vma=False,
    )
```
